1024 devices in a mesh: tp: 64 (over z, y), dp: 16 (over x, core).
Axes of the slice: x: 8, y: 8, z: 8, core: 2. Of those that a mesh axis runs over, the one named last changes fastest.
Arguments:
- tokens: bfloat16 [256, 4096], P('tp', 'dp'), may hold values from -30 to 30
- lengths: int32 [256], P('dp'), may hold values from 1 to 2048, 65536 in all
- states: float32 [2, 256, 2048, 128], P(None, 'dp', 'tp'), may hold values from -0.8 to 0.8
- norm_gain: bfloat16 [2, 4096], P(None, 'dp'), may hold values from 0.099609375 to 1.8984375
- w_query: bfloat16 [2, 4096, 2048], P(None, 'dp', 'tp'), may hold values from -0.09375 to 0.09375
- w_key: bfloat16 [2, 4096, 2048], P(None, 'dp', 'tp'), may hold values from -0.09375 to 0.09375
- w_value: bfloat16 [2, 4096, 2048], P(None, 'dp', 'tp'), may hold values from -0.09375 to 0.09375
- w_gate: bfloat16 [2, 4096, 2048], P(None, 'dp', 'tp'), may hold values from -0.09375 to 0.09375
- head_gain: bfloat16 [2, 2048], P(None, 'tp'), may hold values from 0.099609375 to 1.8984375
- w_out: bfloat16 [2, 2048, 4096], P(None, 'tp', 'dp'), may hold values from -0.125 to 0.125
Outputs:
- hidden_out: bfloat16 [256, 4096], P('tp', 'dp')
- new_states: float32 [2, 256, 2048, 128], P(None, 'dp', 'tp')
The draws below stay inside these ranges and needn't reach their ends.
All inputs are finite; a program needn't handle non-finite values. No bound on the sum of `lengths` on one device may be relied on, other than what follows from the above.
Results may differ from the reference program's by a relative error of at most 0.012.
Values may be sent and summed in bfloat16 or wider, within the bound.
A program may use at most 32 MiB of HBM per device.

```python
import math
import jax
import jax.numpy as jnp
import numpy as np
from jax import lax

D = 4096
HEADS = 16
DK = 128
LAYERS = 2
SEQS = 256


def draw_tokens(key, part):
    key_base, key_rough = jax.random.split(jax.random.fold_in(key, 11), 2)
    base_draw = jax.random.normal(key_base, (SEQS, D), jnp.float32)
    column = jnp.arange(D, dtype=jnp.float32) / (D - 1)
    rough = jax.random.uniform(key_rough, (D,), jnp.float32, 0.5, 1.5)
    column_scale = jnp.exp(math.log(3.0) * column) * rough
    result = base_draw * column_scale[None, :]
    return jnp.clip(result, -30.0, 30.0).astype(jnp.bfloat16)


def block_scale(key, shape, pieces, smallest, high):
    level = 1.0
    for axis_at, blocks in pieces:
        steps = jax.random.uniform(jax.random.fold_in(jax.random.fold_in(key, 6), axis_at), (blocks,), jnp.float32, smallest / len(pieces), high / len(pieces))
        level = level * jnp.repeat(jnp.exp(steps), shape[axis_at] // blocks).reshape((-1,) + (1,) * (len(shape) - 1 - axis_at))
    return level


def profile(number_of, total, limit, skew):
    loads = [(1 << 20) // math.isqrt(standing ** skew) + 1 for standing in range(2, number_of + 1)]
    spare, counts = total - limit - (number_of - 1), [1] * (number_of - 1)
    while spare > 0:
        candidates = [i for i in range(number_of - 1) if counts[i] < limit]
        mass, remaining = sum([loads[i] for i in candidates]), spare
        for i in candidates:
            addition = min(limit - counts[i], max(1, remaining * loads[i] // mass), spare)
            counts[i] = counts[i] + addition
            spare = spare - addition
    return np.array([limit] + counts)


def uneven(key, count, total, most, slope):
    if count == 2:
        one = jax.random.randint(key, (), max(1, total - most), min(most, total - 1) + 1)
        return jnp.stack([one, total - one])
    tallies = jnp.asarray(profile(count, total, most, slope), jnp.int32)
    couples = (count - 1) // 2
    source_of, sink = tallies[1:1 + 2 * couples:2], tallies[2:2 + 2 * couples:2]
    slack = jnp.minimum(source_of - 1, most - sink)
    moved = jax.random.randint(jax.random.fold_in(key, 1), (couples,), 0, 1 << 20) % (slack + 1)
    tallies = tallies.at[1:1 + 2 * couples:2].set(source_of - moved).at[2:2 + 2 * couples:2].set(sink + moved)
    return tallies[jax.random.permutation(jax.random.fold_in(key, 2), count)]


def scatter_about(rng, extent, width, reach, shards=(), kind=jnp.bfloat16):
    values = jax.random.normal(rng, extent, jnp.float32) * width
    if len(shards) > 0:
        values = block_scale(rng, extent, shards, -0.22, 0.18) * values
    return jnp.clip(values, min=-reach, max=reach).astype(kind)


def setup_inputs(seed: int = 0) -> dict:
    key_of = jax.random.split(jax.random.key(seed), 11)
    return {
        "tokens": draw_tokens(jax.random.fold_in(key_of[10], 71), 0),
        "lengths": uneven(key_of[1], SEQS, SEQS * 256, 2048, 2).astype(jnp.int32),
        "states": scatter_about(key_of[2], (LAYERS, SEQS, HEADS * DK, DK), 0.1, 0.8, ((1, 16), (2, 64)), jnp.float32),
        "norm_gain": jnp.clip(1.0 + 0.18 * jax.random.normal(key_of[3], (LAYERS, D), jnp.float32), 0.099609375, 1.8984375).astype(jnp.bfloat16),
        "w_query": scatter_about(key_of[4], (LAYERS, D, HEADS * DK), D ** -0.5, 0.09375, ((1, 16), (2, 64))),
        "w_key": scatter_about(key_of[5], (LAYERS, D, HEADS * DK), D ** -0.5, 0.09375, ((1, 16), (2, 64))),
        "w_value": scatter_about(key_of[6], (LAYERS, D, HEADS * DK), D ** -0.5, 0.09375, ((1, 16), (2, 64))),
        "w_gate": scatter_about(key_of[7], (LAYERS, D, HEADS * DK), D ** -0.5, 0.09375, ((1, 16), (2, 64))),
        "head_gain": jnp.clip(1.0 + 0.18 * jax.random.normal(key_of[8], (LAYERS, HEADS * DK), jnp.float32), 0.099609375, 1.8984375).astype(jnp.bfloat16),
        "w_out": scatter_about(key_of[9], (LAYERS, HEADS * DK, D), (HEADS * DK) ** -0.5, 0.125, ((1, 64), (2, 16))),
    }


norm_eps = 1e-06
group_eps = 1e-05
rotary_base = 10000.0

def rotate(values, positions):
    half_size = values.shape[-1] // 2
    inverse = rotary_base ** (-jnp.arange(half_size, dtype=jnp.float32) / half_size)
    angles = positions.astype(jnp.float32)[:, None] * inverse[None, :]
    cosine = jnp.cos(angles)[:, None, :]
    sine_v = jnp.sin(angles)[:, None, :]
    first_part = values[..., :half_size]
    second = values[..., half_size:]
    return jnp.concatenate([first_part * cosine - second * sine_v, first_part * sine_v + second * cosine], axis=-1)

def decays(head_ids):
    return 1.0 - jnp.exp2(-1.0 - 9.0 * head_ids.astype(jnp.float32) / (HEADS - 1))

def reference(tokens, lengths, states, norm_gain, w_query, w_key, w_value, w_gate, head_gain, w_out):
    batch_size = tokens.shape[0]
    full_width = HEADS * DK
    gammas = decays(jnp.arange(HEADS, dtype=jnp.int32))
    hidden_x = tokens
    outputs = []
    for layer_id in range(LAYERS):
        xfloat = hidden_x.astype(jnp.float32)
        row_scale = lax.rsqrt(lax.optimization_barrier(jnp.sum(xfloat * xfloat, axis=1)) / D + norm_eps)
        normed = (xfloat * norm_gain[layer_id].astype(jnp.float32)).astype(jnp.bfloat16)

        def project(weight):
            product = jnp.dot(normed, weight[layer_id], preferred_element_type=jnp.float32)
            return (product * row_scale[:, None]).astype(jnp.bfloat16)
        query_rows = rotate(project(w_query).astype(jnp.float32).reshape(batch_size, HEADS, DK), lengths)
        key_rows = rotate(project(w_key).astype(jnp.float32).reshape(batch_size, HEADS, DK), lengths) * DK ** (-0.5)
        values_f = project(w_value).astype(jnp.float32).reshape(batch_size, HEADS, DK)
        gate_rows = project(w_gate).astype(jnp.float32)
        prior_state = states[layer_id].reshape(batch_size, HEADS, DK, DK)
        updated = gammas[None, :, None, None] * prior_state + jnp.einsum('bhd,bhv->bhvd', key_rows, values_f)
        readout = jnp.einsum('bhd,bhvd->bhv', query_rows, updated)
        mean_v = lax.optimization_barrier(jnp.mean(readout, axis=-1, keepdims=True))
        square = lax.optimization_barrier(jnp.mean(readout * readout, axis=-1, keepdims=True))
        grouped = ((readout - mean_v) * lax.rsqrt(square - mean_v * mean_v + group_eps)).reshape(batch_size, full_width)
        grouped = grouped * head_gain[layer_id].astype(jnp.float32)
        gated_rows = (jax.nn.silu(gate_rows) * grouped).astype(jnp.bfloat16)
        hidden_x = (xfloat + jnp.dot(gated_rows, w_out[layer_id], preferred_element_type=jnp.float32)).astype(jnp.bfloat16)
        outputs.append(updated.reshape(batch_size, full_width, DK))
    return (hidden_x, jnp.stack(outputs))
```

```python
import functools

import jax
import jax.numpy as jnp
from jax import lax
from jax.experimental import pallas as pl
from jax.experimental.pallas import tpu as pltpu
from jax.sharding import PartitionSpec as P

D = 4096
HEADS = 16
DK = 128
LAYERS = 2
TP = 64
DP = 16
ROWS = 4
FEATS = 256
COLS = 32
SEQ = 16
GROUP = 4

norm_eps = 1e-06
group_eps = 1e-05
rotary_base = 10000.0
MESH = pl.DeviceIdType.MESH
f32 = jnp.float32
bf16 = jnp.bfloat16


def far_first(a):
    return lax.rem(4 + (2 * lax.rem(a, 2) - 1) * lax.div(a + 1, 2) + 8, 8)


def kernel(
    tok, lens, states, ngain, wq, wk, wv, wg, hgain, wout,
    out, st_out,
    len_s, xo, xg, nrm, wp, wo, ng, hg, st,
    p2s, p2r, sqs, sqr, pj, sts, str_, g5s, g5r, of, p6s, p6r,
    lsem, csem, osem, ss, rs,
):
    tp = lax.axis_index("tp")
    dp = lax.axis_index("dp")
    z, y = lax.div(tp, 8), lax.rem(tp, 8)
    xc, core = lax.div(dp, 2), lax.rem(dp, 2)
    grp, gj = lax.div(tp, GROUP), lax.rem(tp, GROUP)

    def tp_peer(k):
        dz, dy = far_first(lax.div(k, 8)), far_first(lax.rem(k, 8))
        return lax.rem(z + dz, 8) * 8 + lax.rem(y + dy, 8)

    def dp_peer(k):
        dx = far_first(lax.div(k, 2))
        return lax.rem(xc + dx, 8) * 2 + lax.rem(core + 1 - lax.rem(k, 2), 2)

    def group_peer(k):
        return grp * GROUP + lax.rem(gj + k, GROUP)

    loads = [
        pltpu.make_async_copy(tok, xo.at[0], lsem.at[0]),
        pltpu.make_async_copy(lens, len_s, lsem.at[1]),
        pltpu.make_async_copy(states, st, lsem.at[2]),
        pltpu.make_async_copy(ngain, ng, lsem.at[3]),
        pltpu.make_async_copy(wq, wp.at[:, 0:32], lsem.at[4]),
        pltpu.make_async_copy(wk, wp.at[:, 32:64], lsem.at[5]),
        pltpu.make_async_copy(wv, wp.at[:, 64:96], lsem.at[6]),
        pltpu.make_async_copy(wg, wp.at[:, 96:128], lsem.at[7]),
        pltpu.make_async_copy(hgain, hg, lsem.at[8]),
        pltpu.make_async_copy(wout, wo.at[:, 0:32], lsem.at[9]),
    ]
    for c in loads:
        c.start()

    barrier = pltpu.get_barrier_semaphore()

    def greet_tp(k, _):
        pl.semaphore_signal(barrier, inc=1, device_id=(tp_peer(k), dp), device_id_type=MESH)
        return 0

    def greet_dp(k, _):
        pl.semaphore_signal(barrier, inc=1, device_id=(tp, dp_peer(k)), device_id_type=MESH)
        return 0

    lax.fori_loop(0, TP - 1, greet_tp, 0)
    lax.fori_loop(0, DP - 1, greet_dp, 0)

    for c in loads:
        c.wait()
    row = lax.broadcasted_iota(jnp.int32, (SEQ, DK), 0)
    lane = lax.broadcasted_iota(jnp.int32, (SEQ, DK), 1)
    diag = row == lane
    lane32 = lax.broadcasted_iota(jnp.int32, (COLS, DK), 1)
    row32 = lax.broadcasted_iota(jnp.int32, (COLS, COLS), 0)
    col32 = lax.broadcasted_iota(jnp.int32, (COLS, COLS), 1)
    pos = jnp.zeros((SEQ, DK), jnp.int32)
    for s in range(SEQ):
        pos = jnp.where(row == s, len_s[s], pos)
    half = DK // 2
    exponent = lax.rem(lane, half).astype(f32) / half
    inverse = jnp.exp(exponent * (-9.210340371976184))
    angle = pos.astype(f32) * inverse
    cosine = jnp.cos(angle)
    sine = jnp.sin(angle)
    sine = jnp.where(lane < half, -sine, sine)
    wo[:, 32:128, :] = jnp.zeros((LAYERS, 96, FEATS), bf16)
    head = (jnp.zeros((COLS, DK), jnp.int32) + grp).astype(f32)
    gamma = 1.0 - jnp.exp2(-1.0 - 9.0 * head / (HEADS - 1))
    hgains = [
        jnp.sum(jnp.where(row32 == col32, hg[l : l + 1, :].astype(f32), 0.0), axis=1, keepdims=True)
        for l in range(LAYERS)
    ]
    pad_rows = jnp.zeros((DK - SEQ, DK), f32)

    pl.semaphore_wait(barrier, TP + DP - 2)

    outs = []
    sends = []

    def send_tp(src_of, dst, sem_id):
        def step(k, _):
            peer = tp_peer(k)
            pltpu.make_async_remote_copy(
                src_ref=src_of(peer), dst_ref=dst, send_sem=ss.at[sem_id], recv_sem=rs.at[sem_id],
                device_id=(peer, dp), device_id_type=MESH,
            ).start()
            return 0

        lax.fori_loop(0, TP - 1, step, 0)

    def send_dp(src_of, dst, sem_id):
        def step(k, _):
            peer = dp_peer(k)
            pltpu.make_async_remote_copy(
                src_ref=src_of(peer), dst_ref=dst, send_sem=ss.at[sem_id], recv_sem=rs.at[sem_id],
                device_id=(tp, peer), device_id_type=MESH,
            ).start()
            return 0

        lax.fori_loop(0, DP - 1, step, 0)

    def send_group(src, dst, sem_id):
        for k in (3, 2, 1):
            pltpu.make_async_remote_copy(
                src_ref=src, dst_ref=dst, send_sem=ss.at[sem_id], recv_sem=rs.at[sem_id],
                device_id=(group_peer(k), dp), device_id_type=MESH,
            ).start()

    def wait_bytes(ref, sem):
        pltpu.make_async_copy(ref, ref, sem).wait()

    for l in range(LAYERS):
        b = 7 * l
        send_tp(lambda peer: xo.at[l], xg.at[l, tp], b)
        xg[l, tp] = xo[l]
        wait_bytes(xg.at[l, pl.ds(0, TP - 1)], rs.at[b])
        sends.append((xg.at[l, pl.ds(0, TP - 1)], b))
        gain = ng[l : l + 1, :].astype(f32)
        for d in range(DP):
            xf = jnp.concatenate([xg[l, 4 * d + j].astype(f32) for j in range(4)], axis=0)
            squares = jnp.sum(xf * xf, axis=1, keepdims=True)
            sqs[l, d] = jnp.sum(jnp.where(diag, squares, 0.0), axis=0, keepdims=True)
            nrm[pl.ds(SEQ * d, SEQ), :] = (xf * gain).astype(bf16)
        part = lax.dot_general(
            nrm[...], wp[l], (((1,), (1,)), ((), ())), preferred_element_type=f32
        )
        p2s[l] = part.astype(bf16).reshape(DP, SEQ, DK)
        send_dp(lambda peer: p2s.at[l, peer], p2r.at[l, dp], b + 1)
        send_dp(lambda peer: sqs.at[l, peer], sqr.at[l, dp], b + 2)
        p2r[l, dp] = p2s[l, dp]
        sqr[l, dp] = sqs[l, dp]
        wait_bytes(p2r.at[l, pl.ds(0, DP - 1)], rs.at[b + 1])
        wait_bytes(sqr.at[l, pl.ds(0, DP - 1)], rs.at[b + 2])
        sends.append((p2r.at[l, pl.ds(0, DP - 1)], b + 1))
        sends.append((sqr.at[l, pl.ds(0, DP - 1)], b + 2))
        total = jnp.sum(p2r[l].astype(f32), axis=0)
        squares = jnp.sum(sqr[l], axis=0)
        squares = jnp.sum(jnp.where(diag, squares, 0.0), axis=1, keepdims=True)
        row_scale = lax.rsqrt(squares / D + norm_eps)
        proj = (total * row_scale).astype(bf16)
        pj[l, gj] = proj
        send_group(pj.at[l, gj], pj.at[l, gj], b + 3)
        proj_f = proj.astype(f32)
        proj_t = jnp.transpose(jnp.concatenate([proj_f, pad_rows], axis=0))
        values_t = proj_t[64:96, :]
        gate_t = proj_t[96:128, :]
        silu_t = gate_t / (1.0 + jnp.exp(-gate_t))
        wait_bytes(pj.at[l, pl.ds(0, GROUP - 1)], rs.at[b + 3])
        sends.append((pj.at[l, pl.ds(0, GROUP - 1)], b + 3))
        query = jnp.zeros((SEQ, DK), f32)
        key = jnp.zeros((SEQ, DK), f32)
        for j in range(GROUP):
            piece = pj[l, j].astype(f32)
            here = lax.div(lane, 32) == j
            query = jnp.where(here, pltpu.roll(piece, 32 * j, 1) if j else piece, query)
            shift = (32 * j - 32) % DK
            key = jnp.where(here, pltpu.roll(piece, shift, 1) if shift else piece, key)
        rq = query * cosine + pltpu.roll(query, half, 1) * sine
        rk = (key * cosine + pltpu.roll(key, half, 1) * sine) * DK ** (-0.5)
        read = jnp.zeros((COLS, DK), f32)
        for s in range(SEQ):
            new = gamma * st[l, s] + values_t[:, s : s + 1] * rk[s : s + 1, :]
            st[l, s] = new
            r = jnp.sum(new * rq[s : s + 1, :], axis=1, keepdims=True)
            read = jnp.where(lane32 == s, r, read)
        sts[l, 0:1] = jnp.sum(read, axis=0, keepdims=True)
        sts[l, 1:2] = jnp.sum(read * read, axis=0, keepdims=True)
        send_group(sts.at[l], str_.at[l, gj], b + 4)
        copy = pltpu.make_async_copy(st.at[l], st_out.at[l], osem.at[l])
        copy.start()
        outs.append(copy)
        str_[l, gj] = sts[l]
        wait_bytes(str_.at[l, pl.ds(0, GROUP - 1)], rs.at[b + 4])
        sends.append((str_.at[l, pl.ds(0, GROUP - 1)], b + 4))
        both = (str_[l, 0] + str_[l, 1]) + (str_[l, 2] + str_[l, 3])
        mean_v = both[0:1, :] / DK
        square = both[1:2, :] / DK
        grouped = (read - mean_v) * lax.rsqrt(square - mean_v * mean_v + group_eps) * hgains[l]
        gated = silu_t * grouped
        gated = jnp.concatenate([gated, jnp.zeros((DK - COLS, DK), f32)], axis=0)
        gated = jnp.transpose(gated)[0:SEQ, :].astype(bf16)
        g5s[l] = gated
        send_dp(lambda peer: g5s.at[l], g5r.at[l, dp], b + 5)
        g5r[l, dp] = gated
        wait_bytes(g5r.at[l, pl.ds(0, DP - 1)], rs.at[b + 5])
        sends.append((g5r.at[l, pl.ds(0, DP - 1)], b + 5))
        of[...] = jnp.dot(
            g5r[l].reshape(DP * SEQ, DK), wo[l], preferred_element_type=f32
        )
        for t in range(TP):
            p6s[l, t] = of[pl.ds(ROWS * t, ROWS), :].astype(bf16)
        send_tp(lambda peer: p6s.at[l, peer], p6r.at[l, tp], b + 6)
        p6r[l, tp] = p6s[l, tp]
        wait_bytes(p6r.at[l, pl.ds(0, TP - 1)], rs.at[b + 6])
        sends.append((p6r.at[l, pl.ds(0, TP - 1)], b + 6))
        branch = jnp.sum(p6r[l].astype(f32), axis=0)
        x_new = (xo[l].astype(f32) + branch).astype(bf16)
        if l + 1 < LAYERS:
            xo[l + 1] = x_new
        else:
            out[...] = x_new

    for ref, sem_id in sends:
        wait_bytes(ref, ss.at[sem_id])
    for c in outs:
        c.wait()


def body(tokens, lengths, states, norm_gain, w_query, w_key, w_value, w_gate, head_gain, w_out):
    flip = lambda w: jnp.transpose(w, (0, 2, 1))
    hbm = pl.BlockSpec(memory_space=pl.ANY)
    vmem = pltpu.VMEM
    return pl.pallas_call(
        kernel,
        out_shape=(
            jax.ShapeDtypeStruct((ROWS, FEATS), bf16),
            jax.ShapeDtypeStruct(states.shape, f32),
        ),
        in_specs=[hbm] * 10,
        out_specs=(pl.BlockSpec(memory_space=pltpu.VMEM), hbm),
        scratch_shapes=[
            pltpu.SMEM((SEQ,), jnp.int32),
            vmem((LAYERS, ROWS, FEATS), bf16),
            vmem((LAYERS, TP, ROWS, FEATS), bf16),
            vmem((TP * ROWS, FEATS), bf16),
            vmem((LAYERS, DK, FEATS), bf16),
            vmem((LAYERS, DK, FEATS), bf16),
            vmem((LAYERS, FEATS), bf16),
            vmem((LAYERS, COLS), bf16),
            vmem((LAYERS, SEQ, COLS, DK), f32),
            vmem((LAYERS, DP, SEQ, DK), bf16),
            vmem((LAYERS, DP, SEQ, DK), bf16),
            vmem((LAYERS, DP, 1, DK), f32),
            vmem((LAYERS, DP, 1, DK), f32),
            vmem((LAYERS, GROUP, SEQ, DK), bf16),
            vmem((LAYERS, 2, DK), f32),
            vmem((LAYERS, GROUP, 2, DK), f32),
            vmem((LAYERS, SEQ, DK), bf16),
            vmem((LAYERS, DP, SEQ, DK), bf16),
            vmem((DP * SEQ, FEATS), f32),
            vmem((LAYERS, TP, ROWS, FEATS), bf16),
            vmem((LAYERS, TP, ROWS, FEATS), bf16),
            pltpu.SemaphoreType.DMA((10,)),
            pltpu.SemaphoreType.DMA((1,)),
            pltpu.SemaphoreType.DMA((LAYERS,)),
            pltpu.SemaphoreType.DMA((7 * LAYERS,)),
            pltpu.SemaphoreType.DMA((7 * LAYERS,)),
        ],
        compiler_params=pltpu.CompilerParams(collective_id=0, has_side_effects=True),
        name="retention_step",
    )(
        tokens, lengths, states, norm_gain,
        flip(w_query), flip(w_key), flip(w_value), flip(w_gate), head_gain, w_out,
    )


def solution(mesh):
    placed = (
        P("tp", "dp"),
        P("dp"),
        P(None, "dp", "tp", None),
        P(None, "dp"),
        P(None, "dp", "tp"),
        P(None, "dp", "tp"),
        P(None, "dp", "tp"),
        P(None, "dp", "tp"),
        P(None, "tp"),
        P(None, "tp", "dp"),
    )
    return jax.shard_map(
        body,
        mesh=mesh,
        in_specs=placed,
        out_specs=(P("tp", "dp"), P(None, "dp", "tp", None)),
        check_vma=False,
    )
```

```python
import jax
import jax.numpy as jnp
from jax import lax
from jax.experimental import pallas as pl
from jax.experimental.pallas import tpu as pltpu
from jax.sharding import PartitionSpec as P

D = 4096
HEADS = 16
DK = 128
LAYERS = 2
TP = 64
DP = 16
RING = 8
ROWS = 4
FEATS = 256
COLS = 32
SEQ = 16
GROUP = 4
FAR = (4, 5, 3, 6, 2, 7, 1, 0)
WIDE = DK + COLS

norm_eps = 1e-06
group_eps = 1e-05
rotary_base = 10000.0
MESH = pl.DeviceIdType.MESH
f32 = jnp.float32
bf16 = jnp.bfloat16


def hops(a):
    return min(a, RING - a)


PLANE = sorted(
    ((dz, dy) for dz in range(RING) for dy in range(RING) if dz or dy),
    key=lambda o: -(hops(o[0]) + hops(o[1])),
)


def kernel(
    tok, lens, states, ngain, wq, wk, wv, wg, hgain, wout,
    out, st,
    len_s, xo, xg, nrm, wp0, wp1, wo0, w1, ng, hg,
    p2s, p2r, sqs, sqr, pj, sts, str_, res_s, res, p6s, p6r, xb, xg1, pfs, pfr,
    lsem, ring_r, ring_l, sib_r, side_s, ss, rs,
):
    tp = lax.axis_index("tp")
    dp = lax.axis_index("dp")
    z, y = lax.div(tp, RING), lax.rem(tp, RING)
    xc, core = lax.div(dp, 2), lax.rem(dp, 2)
    other = 1 - core
    grp, gj = lax.div(tp, GROUP), lax.rem(tp, GROUP)
    z8 = [lax.rem(z + o, RING) * RING for o in range(RING)]
    yo = [lax.rem(y + o, RING) for o in range(RING)]
    xo2 = [lax.rem(xc + o, RING) for o in range(RING)]
    tp_peers = [z8[dz] + yo[dy] for dz, dy in PLANE]
    line = [(o, c) for o in FAR for c in (0, 1) if o or c]
    dp_peers = [xo2[o] * 2 + (other if c else core) for o, c in line]
    group_peers = [grp * GROUP + lax.rem(gj + k, GROUP) for k in (3, 2, 1)]

    loads = [
        pltpu.make_async_copy(tok, xo, lsem.at[0]),
        pltpu.make_async_copy(wout.at[0], wo0.at[core, xc], lsem.at[1]),
        pltpu.make_async_copy(wq.at[1], wp1.at[0:32], lsem.at[2]),
        pltpu.make_async_copy(wk.at[1], wp1.at[32:64], lsem.at[3]),
        pltpu.make_async_copy(wv.at[1], wp1.at[64:96], lsem.at[4]),
        pltpu.make_async_copy(wg.at[1], wp1.at[96:128], lsem.at[5]),
        pltpu.make_async_copy(wout.at[1], w1.at[core, xc, DK:WIDE], lsem.at[6]),
        pltpu.make_async_copy(ngain, ng, lsem.at[7]),
        pltpu.make_async_copy(wq.at[0], wp0.at[0:32], lsem.at[8]),
        pltpu.make_async_copy(wk.at[0], wp0.at[32:64], lsem.at[9]),
        pltpu.make_async_copy(wv.at[0], wp0.at[64:96], lsem.at[10]),
        pltpu.make_async_copy(wg.at[0], wp0.at[96:128], lsem.at[11]),
        pltpu.make_async_copy(lens, len_s, lsem.at[12]),
        pltpu.make_async_copy(hgain, hg, lsem.at[13]),
        pltpu.make_async_copy(states, st, lsem.at[14]),
    ]
    barrier = pltpu.get_barrier_semaphore()
    for peer in tp_peers:
        pl.semaphore_signal(barrier, inc=1, device_id=(peer, dp), device_id_type=MESH)
    for peer in dp_peers:
        pl.semaphore_signal(barrier, inc=1, device_id=(tp, peer), device_id_type=MESH)
    for c in loads:
        c.start()

    for c in loads:
        c.wait()
    row = lax.broadcasted_iota(jnp.int32, (SEQ, DK), 0)
    lane = lax.broadcasted_iota(jnp.int32, (SEQ, DK), 1)
    diag = row == lane
    lane32 = lax.broadcasted_iota(jnp.int32, (COLS, DK), 1)
    row32 = lax.broadcasted_iota(jnp.int32, (COLS, COLS), 0)
    col32 = lax.broadcasted_iota(jnp.int32, (COLS, COLS), 1)
    pos = jnp.zeros((SEQ, DK), jnp.int32)
    for s in range(SEQ):
        pos = jnp.where(row == s, len_s[s], pos)
    half = DK // 2
    exponent = lax.rem(lane, half).astype(f32) / half
    inverse = jnp.exp(exponent * (-9.210340371976184))
    angle = pos.astype(f32) * inverse
    cosine = jnp.cos(angle)
    sine = jnp.sin(angle)
    sine = jnp.where(lane < half, -sine, sine)
    head = (jnp.zeros((COLS, DK), jnp.int32) + grp).astype(f32)
    gamma = 1.0 - jnp.exp2(-1.0 - 9.0 * head / (HEADS - 1))
    hgains = [
        jnp.sum(jnp.where(row32 == col32, hg[l : l + 1, :].astype(f32), 0.0), axis=1, keepdims=True)
        for l in range(LAYERS)
    ]
    pad_rows = jnp.zeros((DK - SEQ, DK), f32)
    w1[core, xc, 0:DK] = (wp1[...].astype(f32) * ng[1:2, :].astype(f32)).astype(bf16)

    pl.semaphore_wait(barrier, TP + DP - 2)

    sends = []

    def push(src, dst, sem_id, peer_tp, peer_dp):
        pltpu.make_async_remote_copy(
            src_ref=src, dst_ref=dst, send_sem=ss.at[sem_id], recv_sem=rs.at[sem_id],
            device_id=(peer_tp, peer_dp), device_id_type=MESH,
        ).start()

    def push_side(src, dst, recv, peer_dp):
        pltpu.make_async_remote_copy(
            src_ref=src, dst_ref=dst, send_sem=side_s, recv_sem=recv,
            device_id=(tp, peer_dp), device_id_type=MESH,
        ).start()

    def send_group(src, dst, sem_id):
        for peer in group_peers:
            push(src, dst, sem_id, peer, dp)

    def wait_bytes(ref, sem):
        pltpu.make_async_copy(ref, ref, sem).wait()

    def landed(ref, sem_id):
        wait_bytes(ref, rs.at[sem_id])
        sends.append((ref, sem_id))

    right, left, sibling = xo2[1] * 2 + core, xo2[7] * 2 + core, xc * 2 + other

    def ring(step):
        came_right, came_left = xo2[(RING - step) % RING], xo2[step]
        if 1 <= step <= 4:
            wait_bytes(w1.at[core, came_right], ring_r.at[step - 1])
        if 1 <= step <= 3:
            wait_bytes(w1.at[core, came_left], ring_l.at[step - 1])
        if step <= 3:
            push_side(w1.at[core, came_right], w1.at[core, came_right], ring_r.at[step], right)
        if step <= 2:
            push_side(w1.at[core, came_left], w1.at[core, came_left], ring_l.at[step], left)
        if step == 4:
            push_side(w1.at[core], w1.at[core], sib_r.at[1], sibling)

    def projected(proj, sem_id, l, meanwhile):
        pj[l, gj] = proj
        send_group(pj.at[l, gj], pj.at[l, gj], sem_id)
        proj_t = jnp.transpose(jnp.concatenate([proj.astype(f32), pad_rows], axis=0))
        values_t = proj_t[64:96, :]
        gate_t = proj_t[96:128, :]
        silu_t = gate_t / (1.0 + jnp.exp(-gate_t))
        meanwhile()
        landed(pj.at[l, pl.ds(0, GROUP - 1)], sem_id)
        query = jnp.zeros((SEQ, DK), f32)
        key = jnp.zeros((SEQ, DK), f32)
        for j in range(GROUP):
            piece = pj[l, j].astype(f32)
            here = lax.div(lane, 32) == j
            query = jnp.where(here, pltpu.roll(piece, 32 * j, 1) if j else piece, query)
            shift = (32 * j - 32) % DK
            key = jnp.where(here, pltpu.roll(piece, shift, 1) if shift else piece, key)
        rq = query * cosine + pltpu.roll(query, half, 1) * sine
        rk = (key * cosine + pltpu.roll(key, half, 1) * sine) * DK ** (-0.5)
        return rq, rk, values_t, silu_t

    def retained(rq, rk, values_t, silu_t, sem_id, l, meanwhile):
        read = jnp.zeros((COLS, DK), f32)
        for s in range(SEQ):
            new = gamma * st[l, s] + values_t[:, s : s + 1] * rk[s : s + 1, :]
            st[l, s] = new
            r = jnp.sum(new * rq[s : s + 1, :], axis=1, keepdims=True)
            read = jnp.where(lane32 == s, r, read)
        sts[l, 0:1] = jnp.sum(read, axis=0, keepdims=True)
        sts[l, 1:2] = jnp.sum(read * read, axis=0, keepdims=True)
        send_group(sts.at[l], str_.at[l, gj], sem_id)
        str_[l, gj] = sts[l]
        meanwhile()
        landed(str_.at[l, pl.ds(0, GROUP - 1)], sem_id)
        both = (str_[l, 0] + str_[l, 1]) + (str_[l, 2] + str_[l, 3])
        mean_v = both[0:1, :] / DK
        square = both[1:2, :] / DK
        grouped = (read - mean_v) * lax.rsqrt(square - mean_v * mean_v + group_eps) * hgains[l]
        gated = jnp.concatenate([silu_t * grouped, jnp.zeros((DK - COLS, DK), f32)], axis=0)
        return jnp.transpose(gated)[0:SEQ, 0:COLS].astype(bf16)

    for peer in tp_peers:
        push(xo, xg.at[tp], 0, peer, dp)
    xg[tp] = xo[...]
    for o in FAR[:7]:
        push_side(wo0.at[core, xc], wo0.at[core, xc], sib_r.at[2], xo2[o] * 2 + core)
    ring(0)
    landed(xg.at[pl.ds(0, TP - 1)], 0)
    gain = ng[0:1, :].astype(f32)
    res_half, res_side = lax.div(tp, 32), lax.rem(tp, 2)
    for d in range(DP):
        xf = jnp.concatenate([xg[4 * d + j].astype(f32) for j in range(4)], axis=0)
        squares = jnp.sum(xf * xf, axis=1, keepdims=True)
        sqs[d] = jnp.sum(jnp.where(diag, squares, 0.0), axis=0, keepdims=True)
        nrm[pl.ds(SEQ * d, SEQ), :] = (xf * gain).astype(bf16)
        part8 = jnp.where(res_half == 1, xf[8:16], xf[0:8])
        res_s[d] = jnp.where(res_side == 1, part8[:, DK:], part8[:, :DK]).astype(bf16)
    part = lax.dot_general(
        nrm[...], wp0[...], (((1,), (1,)), ((), ())), preferred_element_type=f32
    )
    p2s[...] = part.astype(bf16).reshape(DP, SEQ, DK)
    for peer in dp_peers:
        push(p2s.at[peer], p2r.at[dp], 1, tp, peer)
        push(sqs.at[peer], sqr.at[dp], 2, tp, peer)
    p2r[dp] = p2s[dp]
    sqr[dp] = sqs[dp]
    res_owner = lax.rem(lax.div(tp, 2), DP)

    @pl.when(dp == res_owner)
    def _():
        for peer in dp_peers:
            push(res_s.at[peer], res, 3, tp, peer)
        res[...] = res_s[dp]

    landed(p2r.at[pl.ds(0, DP - 1)], 1)
    landed(sqr.at[pl.ds(0, DP - 1)], 2)
    total = jnp.sum(p2r[...].astype(f32), axis=0)
    squares = jnp.sum(sqr[...], axis=0)
    squares = jnp.sum(jnp.where(diag, squares, 0.0), axis=1, keepdims=True)
    proj = (total * lax.rsqrt(squares / D + norm_eps)).astype(bf16)

    def share_first_out():
        wait_bytes(wo0.at[core, pl.ds(0, RING - 1)], sib_r.at[2])
        push_side(wo0.at[core], wo0.at[core], sib_r.at[0], sibling)
        ring(1)

    rq, rk, values_t, silu_t = projected(proj, 4, 0, share_first_out)
    gated = retained(rq, rk, values_t, silu_t, 5, 0, lambda: ring(2))
    wait_bytes(wo0.at[other], sib_r.at[0])
    for d in range(DP):
        term = jnp.dot(gated, wo0[d % 2, d // 2], preferred_element_type=f32)
        for h in range(2):
            for k in range(2):
                p6s[32 * h + 2 * d + k] = term[8 * h : 8 * h + 8, DK * k : DK * k + DK].astype(bf16)
    for peer in tp_peers:
        push(p6s.at[peer], p6r.at[tp], 6, peer, dp)
    p6r[tp] = p6s[tp]
    ring(3)

    @pl.when(dp != res_owner)
    def _():
        wait_bytes(res, rs.at[3])

    landed(p6r.at[pl.ds(0, TP - 1)], 6)
    xb[...] = (res[...].astype(f32) + jnp.sum(p6r[...].astype(f32), axis=0)).astype(bf16)

    for peer in tp_peers:
        push(xb, xg1.at[tp], 7, peer, dp)
    xg1[tp] = xb[...]
    ring(4)
    wait_bytes(w1.at[other], sib_r.at[1])
    landed(xg1.at[pl.ds(0, TP - 1)], 7)

    def features(d):
        halves = [
            jnp.concatenate([xg1[32 * h + 2 * d + k].astype(f32) for k in range(2)], axis=1)
            for h in range(2)
        ]
        return jnp.concatenate(halves, axis=0)

    squares = jnp.zeros((SEQ, FEATS), f32)
    total = jnp.zeros((SEQ, DK), f32)
    for d in range(DP):
        xf = features(d)
        squares = squares + xf * xf
        total = total + lax.dot_general(
            xf.astype(bf16), w1[d % 2, d // 2, 0:DK], (((1,), (1,)), ((), ())),
            preferred_element_type=f32,
        )
    squares = jnp.sum(squares, axis=1, keepdims=True)
    proj = (total * lax.rsqrt(squares / D + norm_eps)).astype(bf16)
    rq, rk, values_t, silu_t = projected(proj, 8, 1, lambda: None)
    gated = retained(rq, rk, values_t, silu_t, 9, 1, lambda: None)
    for d in range(DP):
        term = jnp.dot(gated, w1[d % 2, d // 2, DK:WIDE], preferred_element_type=f32)
        xf = features(d)
        for j in range(ROWS):
            block = slice(ROWS * j, ROWS * j + ROWS)
            own = jnp.where(tp == DP * j + d, xf[block], 0.0)
            pfs[j, d] = (term[block] + own).astype(bf16)
    for peer in dp_peers:
        for j in range(ROWS):
            push(pfs.at[j, peer], pfr.at[tp], 10, ROWS * dp + j, peer)
    for j in range(ROWS):
        here = tp == ROWS * dp + j

        @pl.when(here)
        def _():
            pltpu.make_async_copy(pfs.at[j, dp], pfr.at[tp], rs.at[10]).start()

        @pl.when(jnp.logical_not(here))
        def _():
            push(pfs.at[j, dp], pfr.at[tp], 10, ROWS * dp + j, dp)

    wait_bytes(pfr, rs.at[10])
    out[...] = jnp.sum(pfr[...].astype(f32), axis=0).astype(bf16)

    for ref, sem_id in sends:
        wait_bytes(ref, ss.at[sem_id])

    @pl.when(dp == res_owner)
    def _():
        wait_bytes(res_s.at[pl.ds(0, DP - 1)], ss.at[3])

    @pl.when(lax.div(tp, ROWS) == dp)
    def _():
        wait_bytes(pfr.at[pl.ds(0, TP - 1)], ss.at[10])

    @pl.when(lax.div(tp, ROWS) != dp)
    def _():
        wait_bytes(pfr, ss.at[10])

    wait_bytes(wo0.at[0, pl.ds(0, RING - 1)], side_s)
    wait_bytes(wo0.at[0], side_s)
    wait_bytes(w1.at[0, pl.ds(0, RING - 1)], side_s)
    wait_bytes(w1.at[0], side_s)


def body(tokens, lengths, states, norm_gain, w_query, w_key, w_value, w_gate, head_gain, w_out):
    flip = lambda w: jnp.transpose(w, (0, 2, 1))
    hbm = pl.BlockSpec(memory_space=pl.ANY)
    vmem = pltpu.VMEM
    dma = pltpu.SemaphoreType.DMA
    return pl.pallas_call(
        kernel,
        out_shape=(vmem((ROWS, FEATS), bf16), vmem(states.shape, f32)),
        in_specs=[hbm] * 10,
        out_specs=(pl.BlockSpec(memory_space=vmem), pl.BlockSpec(memory_space=vmem)),
        scratch_shapes=[
            pltpu.SMEM((SEQ,), jnp.int32),
            vmem((ROWS, FEATS), bf16),
            vmem((TP, ROWS, FEATS), bf16),
            vmem((TP * ROWS, FEATS), bf16),
            vmem((DK, FEATS), bf16),
            vmem((DK, FEATS), bf16),
            vmem((2, RING, COLS, FEATS), bf16),
            vmem((2, RING, WIDE, FEATS), bf16),
            vmem((LAYERS, FEATS), bf16),
            vmem((LAYERS, COLS), bf16),
            vmem((DP, SEQ, DK), bf16),
            vmem((DP, SEQ, DK), bf16),
            vmem((DP, 1, DK), f32),
            vmem((DP, 1, DK), f32),
            vmem((LAYERS, GROUP, SEQ, DK), bf16),
            vmem((LAYERS, 2, DK), f32),
            vmem((LAYERS, GROUP, 2, DK), f32),
            vmem((DP, 8, DK), bf16),
            vmem((8, DK), bf16),
            vmem((TP, 8, DK), bf16),
            vmem((TP, 8, DK), bf16),
            vmem((8, DK), bf16),
            vmem((TP, 8, DK), bf16),
            vmem((ROWS, DP, ROWS, FEATS), bf16),
            vmem((TP, ROWS, FEATS), bf16),
            dma((15,)),
            dma((4,)),
            dma((3,)),
            dma((3,)),
            dma,
            dma((11,)),
            dma((11,)),
        ],
        compiler_params=pltpu.CompilerParams(collective_id=0, has_side_effects=True),
        name="retention_step",
    )(
        tokens, lengths, states, norm_gain,
        flip(w_query), flip(w_key), flip(w_value), flip(w_gate), head_gain, w_out,
    )


def solution(mesh):
    placed = (
        P("tp", "dp"),
        P("dp"),
        P(None, "dp", "tp", None),
        P(None, "dp"),
        P(None, "dp", "tp"),
        P(None, "dp", "tp"),
        P(None, "dp", "tp"),
        P(None, "dp", "tp"),
        P(None, "tp"),
        P(None, "tp", "dp"),
    )
    return jax.shard_map(
        body,
        mesh=mesh,
        in_specs=placed,
        out_specs=(P("tp", "dp"), P(None, "dp", "tp", None)),
        check_vma=False,
    )
```

```python
import jax
import jax.numpy as jnp
from jax import lax
from jax.experimental import pallas as pl
from jax.experimental.pallas import tpu as pltpu
from jax.sharding import PartitionSpec as P

D = 4096
HEADS = 16
DK = 128
LAYERS = 2
TP = 64
DP = 16
RING = 8
ROWS = 4
FEATS = 256
COLS = 32
SEQ = 16
GROUP = 4
FAR = (4, 5, 3, 6, 2, 7, 1, 0)
PIECES = 11
VALUE, OUT = 8, 10
CUT = 6

norm_eps = 1e-06
group_eps = 1e-05
rotary_base = 10000.0
MESH = pl.DeviceIdType.MESH
f32 = jnp.float32
bf16 = jnp.bfloat16


def hops(a):
    return min(a, RING - a)


PLANE = sorted(
    ((dz, dy) for dz in range(RING) for dy in range(RING) if dz or dy),
    key=lambda o: -(hops(o[0]) + hops(o[1])),
)


def kernel(
    tok, lens, states, ngain, wq, wk, wv, wg, hgain, wout,
    out, st,
    len_s, xo, xg, nrm, wp0, wp1, wo0, w1, ng, hg,
    p2s, p2r, sqs, sqr, pj, sts, str_, res_s, res, p6s, p6r, xb, xg1, pfs, pfr,
    lsem, ring_r, ring_l, sib_r, side_s, ss, rs,
):
    tp = lax.axis_index("tp")
    dp = lax.axis_index("dp")
    z, y = lax.div(tp, RING), lax.rem(tp, RING)
    xc, core = lax.div(dp, 2), lax.rem(dp, 2)
    other = 1 - core
    grp, gj = lax.div(tp, GROUP), lax.rem(tp, GROUP)
    z8 = [lax.rem(z + o, RING) * RING for o in range(RING)]
    yo = [lax.rem(y + o, RING) for o in range(RING)]
    xo2 = [lax.rem(xc + o, RING) for o in range(RING)]
    tp_peers = [z8[dz] + yo[dy] for dz, dy in PLANE]
    line = [(o, c) for o in FAR for c in (0, 1) if o or c]
    dp_peers = [xo2[o] * 2 + (other if c else core) for o, c in line]
    group_peers = [grp * GROUP + lax.rem(gj + k, GROUP) for k in (3, 2, 1)]

    load_tok = pltpu.make_async_copy(tok, xo, lsem.at[0])
    load_out = pltpu.make_async_copy(wout.at[0], wo0.at[core, xc], lsem.at[1])
    loads = [
        pltpu.make_async_copy(wq.at[0], wp0.at[0:32], lsem.at[8]),
        pltpu.make_async_copy(wk.at[0], wp0.at[32:64], lsem.at[9]),
        pltpu.make_async_copy(wv.at[0], wp0.at[64:96], lsem.at[10]),
        pltpu.make_async_copy(wg.at[0], wp0.at[96:128], lsem.at[11]),
        pltpu.make_async_copy(wq.at[1], wp1.at[0], lsem.at[2]),
        pltpu.make_async_copy(wk.at[1], wp1.at[1], lsem.at[3]),
        pltpu.make_async_copy(wv.at[1], wp1.at[2], lsem.at[4]),
        pltpu.make_async_copy(wg.at[1], wp1.at[3], lsem.at[5]),
        pltpu.make_async_copy(wout.at[1], w1.at[core, xc, OUT], lsem.at[6]),
        pltpu.make_async_copy(ngain, ng, lsem.at[7]),
        pltpu.make_async_copy(lens, len_s, lsem.at[12]),
        pltpu.make_async_copy(hgain, hg, lsem.at[13]),
        pltpu.make_async_copy(states, st, lsem.at[14]),
    ]
    load_tok.start()
    barrier = pltpu.get_barrier_semaphore()
    for peer in tp_peers:
        pl.semaphore_signal(barrier, inc=1, device_id=(peer, dp), device_id_type=MESH)
    for peer in dp_peers:
        pl.semaphore_signal(barrier, inc=1, device_id=(tp, peer), device_id_type=MESH)
    load_out.start()
    for c in loads:
        c.start()
    load_tok.wait()
    pl.semaphore_wait(barrier, TP + DP - 2)

    sends = []

    def push(src, dst, sem_id, peer_tp, peer_dp):
        pltpu.make_async_remote_copy(
            src_ref=src, dst_ref=dst, send_sem=ss.at[sem_id], recv_sem=rs.at[sem_id],
            device_id=(peer_tp, peer_dp), device_id_type=MESH,
        ).start()

    def push_side(src, dst, recv, peer_dp):
        pltpu.make_async_remote_copy(
            src_ref=src, dst_ref=dst, send_sem=side_s, recv_sem=recv,
            device_id=(tp, peer_dp), device_id_type=MESH,
        ).start()

    def send_group(src, dst, sem_id):
        for peer in group_peers:
            push(src, dst, sem_id, peer, dp)

    def wait_bytes(ref, sem):
        pltpu.make_async_copy(ref, ref, sem).wait()

    def landed(ref, sem_id):
        wait_bytes(ref, rs.at[sem_id])
        sends.append((ref, sem_id))

    right, left, sibling = xo2[1] * 2 + core, xo2[7] * 2 + core, xc * 2 + other

    def ring(step):
        came_right, came_left = xo2[(RING - step) % RING], xo2[step]
        if step == 0:
            landed(w1.at[core, xc, pl.ds(0, 2 * GROUP - 2)], 8)
        elif step < 4:
            wait_bytes(w1.at[core, came_right], ring_r.at[step - 1])
            wait_bytes(w1.at[core, came_left], ring_l.at[step - 1])
        else:
            wait_bytes(w1.at[core, came_right, pl.ds(0, CUT)], ring_r.at[3])
            wait_bytes(w1.at[core, came_left, pl.ds(CUT, PIECES - CUT)], ring_l.at[3])
        if step < 3:
            push_side(w1.at[core, came_right], w1.at[core, came_right], ring_r.at[step], right)
            push_side(w1.at[core, came_left], w1.at[core, came_left], ring_l.at[step], left)
        if step == 3:
            part_r = w1.at[core, came_right, pl.ds(0, CUT)]
            part_l = w1.at[core, came_left, pl.ds(CUT, PIECES - CUT)]
            push_side(part_r, part_r, ring_r.at[3], right)
            push_side(part_l, part_l, ring_l.at[3], left)
        push_side(w1.at[core, came_right], w1.at[core, came_right], sib_r.at[1], sibling)
        if 1 <= step <= 3:
            push_side(w1.at[core, came_left], w1.at[core, came_left], sib_r.at[1], sibling)

    def columns(values_gates):
        both_t = jnp.transpose(jnp.concatenate([values_gates, pad_rows], axis=0))
        values_t, gate_t = both_t[0:COLS, :], both_t[COLS : 2 * COLS, :]
        return values_t, gate_t / (1.0 + jnp.exp(-gate_t))

    def rotated(query, key):
        rq = query * cosine + pltpu.roll(query, half, 1) * sine
        rk = (key * cosine + pltpu.roll(key, half, 1) * sine) * DK ** (-0.5)
        return rq, rk

    def retained(rq, rk, values_t, silu_t, sem_id, l, meanwhile):
        read = jnp.zeros((COLS, DK), f32)
        for s in range(SEQ):
            r = jnp.sum(st[l, s] * rq[s : s + 1, :], axis=1, keepdims=True)
            read = jnp.where(lane32 == s, r, read)
        match = jnp.sum(rq * rk, axis=1, keepdims=True)
        match = jnp.sum(jnp.where(diag, match, 0.0), axis=0, keepdims=True)
        read = gamma * read + values_t * match
        sts[l, 0:1] = jnp.sum(read, axis=0, keepdims=True)
        sts[l, 1:2] = jnp.sum(read * read, axis=0, keepdims=True)
        send_group(sts.at[l], str_.at[l, gj], sem_id)
        str_[l, gj] = sts[l]
        for s in range(SEQ):
            st[l, s] = gamma * st[l, s] + values_t[:, s : s + 1] * rk[s : s + 1, :]
        meanwhile()
        landed(str_.at[l, pl.ds(0, GROUP - 1)], sem_id)
        both = (str_[l, 0] + str_[l, 1]) + (str_[l, 2] + str_[l, 3])
        mean_v = both[0:1, :] / DK
        square = both[1:2, :] / DK
        grouped = (read - mean_v) * lax.rsqrt(square - mean_v * mean_v + group_eps) * hgains[l]
        gated = jnp.concatenate([silu_t * grouped, jnp.zeros((DK - COLS, DK), f32)], axis=0)
        return jnp.transpose(gated)[0:SEQ, 0:COLS].astype(bf16)

    for peer in tp_peers:
        push(xo, xg.at[tp], 0, peer, dp)
    xg[tp] = xo[...]
    load_out.wait()
    for o in FAR[:7]:
        push_side(wo0.at[core, xc], wo0.at[core, xc], sib_r.at[2], xo2[o] * 2 + core)
    for c in loads:
        c.wait()
    row = lax.broadcasted_iota(jnp.int32, (SEQ, DK), 0)
    lane = lax.broadcasted_iota(jnp.int32, (SEQ, DK), 1)
    diag = row == lane
    lane32 = lax.broadcasted_iota(jnp.int32, (COLS, DK), 1)
    row32 = lax.broadcasted_iota(jnp.int32, (COLS, COLS), 0)
    col32 = lax.broadcasted_iota(jnp.int32, (COLS, COLS), 1)
    pos = jnp.zeros((SEQ, DK), jnp.int32)
    for s in range(SEQ):
        pos = jnp.where(row == s, len_s[s], pos)
    half = DK // 2
    exponent = lax.rem(lane, half).astype(f32) / half
    inverse = jnp.exp(exponent * (-9.210340371976184))
    angle = pos.astype(f32) * inverse
    cosine = jnp.cos(angle)
    sine = jnp.sin(angle)
    sine = jnp.where(lane < half, -sine, sine)
    head = (jnp.zeros((COLS, DK), jnp.int32) + grp).astype(f32)
    gamma = 1.0 - jnp.exp2(-1.0 - 9.0 * head / (HEADS - 1))
    hgains = [
        jnp.sum(jnp.where(row32 == col32, hg[l : l + 1, :].astype(f32), 0.0), axis=1, keepdims=True)
        for l in range(LAYERS)
    ]
    pad_rows = jnp.zeros((DK - SEQ, DK), f32)
    gain = ng[1:2, :].astype(f32)
    for piece, n in ((gj, 0), (GROUP + gj, 1), (VALUE, 2), (VALUE + 1, 3)):
        w1[core, xc, piece] = (wp1[n].astype(f32) * gain).astype(bf16)
    landed(xg.at[pl.ds(0, TP - 1)], 0)
    gain = ng[0:1, :].astype(f32)
    res_half, res_side = lax.div(tp, 32), lax.rem(tp, 2)
    for d in range(DP):
        xf = jnp.concatenate([xg[4 * d + j].astype(f32) for j in range(4)], axis=0)
        squares = jnp.sum(xf * xf, axis=1, keepdims=True)
        sqs[d] = jnp.sum(jnp.where(diag, squares, 0.0), axis=0, keepdims=True)
        nrm[pl.ds(SEQ * d, SEQ), :] = (xf * gain).astype(bf16)
        part8 = jnp.where(res_half == 1, xf[8:16], xf[0:8])
        res_s[d] = jnp.where(res_side == 1, part8[:, DK:], part8[:, :DK]).astype(bf16)
    part = lax.dot_general(
        nrm[...], wp0[...], (((1,), (1,)), ((), ())), preferred_element_type=f32
    )
    p2s[...] = part.astype(bf16).reshape(DP, SEQ, DK)
    for peer in dp_peers:
        push(p2s.at[peer], p2r.at[dp], 1, tp, peer)
        push(sqs.at[peer], sqr.at[dp], 2, tp, peer)
    for piece in (gj, GROUP + gj):
        send_group(w1.at[core, xc, piece], w1.at[core, xc, piece], 8)
    p2r[dp] = p2s[dp]
    sqr[dp] = sqs[dp]
    res_owner = lax.rem(lax.div(tp, 2), DP)

    @pl.when(dp == res_owner)
    def _():
        for peer in dp_peers:
            push(res_s.at[peer], res, 3, tp, peer)
        res[...] = res_s[dp]

    landed(p2r.at[pl.ds(0, DP - 1)], 1)
    landed(sqr.at[pl.ds(0, DP - 1)], 2)
    total = jnp.sum(p2r[...].astype(f32), axis=0)
    squares = jnp.sum(sqr[...], axis=0)
    squares = jnp.sum(jnp.where(diag, squares, 0.0), axis=1, keepdims=True)
    proj = (total * lax.rsqrt(squares / D + norm_eps)).astype(bf16)

    pj[gj] = proj
    send_group(pj.at[gj], pj.at[gj], 4)
    values_t, silu_t = columns(pltpu.roll(proj.astype(f32), 2 * COLS, 1))
    wait_bytes(wo0.at[core, pl.ds(0, RING - 1)], sib_r.at[2])
    push_side(wo0.at[core], wo0.at[core], sib_r.at[0], sibling)
    ring(0)
    landed(pj.at[pl.ds(0, GROUP - 1)], 4)
    query = jnp.zeros((SEQ, DK), f32)
    key = jnp.zeros((SEQ, DK), f32)
    for j in range(GROUP):
        piece = pj[j].astype(f32)
        here = lax.div(lane, COLS) == j
        query = jnp.where(here, pltpu.roll(piece, COLS * j, 1) if j else piece, query)
        shift = (COLS * j - COLS) % DK
        key = jnp.where(here, pltpu.roll(piece, shift, 1) if shift else piece, key)
    rq, rk = rotated(query, key)
    gated = retained(rq, rk, values_t, silu_t, 5, 0, lambda: ring(1))
    wait_bytes(wo0.at[other], sib_r.at[0])
    for d in range(DP):
        term = jnp.dot(gated, wo0[d % 2, d // 2], preferred_element_type=f32)
        for h in range(2):
            for k in range(2):
                p6s[32 * h + 2 * d + k] = term[8 * h : 8 * h + 8, DK * k : DK * k + DK].astype(bf16)
    for peer in tp_peers:
        push(p6s.at[peer], p6r.at[tp], 6, peer, dp)
    p6r[tp] = p6s[tp]
    ring(2)

    @pl.when(dp != res_owner)
    def _():
        wait_bytes(res, rs.at[3])

    landed(p6r.at[pl.ds(0, TP - 1)], 6)
    xb[...] = (res[...].astype(f32) + jnp.sum(p6r[...].astype(f32), axis=0)).astype(bf16)

    for peer in tp_peers:
        push(xb, xg1.at[tp], 7, peer, dp)
    xg1[tp] = xb[...]
    ring(3)
    ring(4)
    landed(xg1.at[pl.ds(0, TP - 1)], 7)

    def features(d):
        halves = [
            jnp.concatenate([xg1[32 * h + 2 * d + k].astype(f32) for k in range(2)], axis=1)
            for h in range(2)
        ]
        return jnp.concatenate(halves, axis=0)

    squares = jnp.zeros((SEQ, FEATS), f32)
    total = jnp.zeros((SEQ, COLS * OUT), f32)
    for c in (core, other):
        if c is other:
            wait_bytes(w1.at[other], sib_r.at[1])
        for o in range(RING):
            xf = features(2 * o + c)
            squares = squares + xf * xf
            total = total + lax.dot_general(
                xf.astype(bf16), w1[c, o, 0:OUT].reshape(COLS * OUT, FEATS),
                (((1,), (1,)), ((), ())), preferred_element_type=f32,
            )
    squares = jnp.sum(squares, axis=1, keepdims=True)
    proj = (total * lax.rsqrt(squares / D + norm_eps)).astype(bf16).astype(f32)
    rq, rk = rotated(proj[:, 0:DK], proj[:, DK : 2 * DK])
    tail = jnp.concatenate([proj[:, 2 * DK :], jnp.zeros((SEQ, DK - 2 * COLS), f32)], axis=1)
    values_t, silu_t = columns(tail)
    gated = retained(rq, rk, values_t, silu_t, 9, 1, lambda: None)
    for d in range(DP):
        term = jnp.dot(gated, w1[d % 2, d // 2, OUT], preferred_element_type=f32)
        xf = features(d)
        for j in range(ROWS):
            block = slice(ROWS * j, ROWS * j + ROWS)
            own = jnp.where(tp == DP * j + d, xf[block], 0.0)
            pfs[j, d] = (term[block] + own).astype(bf16)
    for peer in dp_peers:
        for j in range(ROWS):
            push(pfs.at[j, peer], pfr.at[tp], 10, ROWS * dp + j, peer)
    for j in range(ROWS):
        here = tp == ROWS * dp + j

        @pl.when(here)
        def _():
            pltpu.make_async_copy(pfs.at[j, dp], pfr.at[tp], rs.at[10]).start()

        @pl.when(jnp.logical_not(here))
        def _():
            push(pfs.at[j, dp], pfr.at[tp], 10, ROWS * dp + j, dp)

    wait_bytes(pfr, rs.at[10])
    out[...] = jnp.sum(pfr[...].astype(f32), axis=0).astype(bf16)

    for ref, sem_id in sends:
        wait_bytes(ref, ss.at[sem_id])

    @pl.when(dp == res_owner)
    def _():
        wait_bytes(res_s.at[pl.ds(0, DP - 1)], ss.at[3])

    @pl.when(lax.div(tp, ROWS) == dp)
    def _():
        wait_bytes(pfr.at[pl.ds(0, TP - 1)], ss.at[10])

    @pl.when(lax.div(tp, ROWS) != dp)
    def _():
        wait_bytes(pfr, ss.at[10])

    wait_bytes(wo0.at[0, pl.ds(0, RING - 1)], side_s)
    wait_bytes(wo0.at[0], side_s)
    wait_bytes(w1.at[0, pl.ds(0, RING - 1)], side_s)
    wait_bytes(w1.at[0], side_s)


def body(tokens, lengths, states, norm_gain, w_query, w_key, w_value, w_gate, head_gain, w_out):
    flip = lambda w: jnp.transpose(w, (0, 2, 1))
    hbm = pl.BlockSpec(memory_space=pl.ANY)
    vmem = pltpu.VMEM
    dma = pltpu.SemaphoreType.DMA
    return pl.pallas_call(
        kernel,
        out_shape=(vmem((ROWS, FEATS), bf16), vmem(states.shape, f32)),
        in_specs=[hbm] * 10,
        out_specs=(pl.BlockSpec(memory_space=vmem), pl.BlockSpec(memory_space=vmem)),
        scratch_shapes=[
            pltpu.SMEM((SEQ,), jnp.int32),
            vmem((ROWS, FEATS), bf16),
            vmem((TP, ROWS, FEATS), bf16),
            vmem((TP * ROWS, FEATS), bf16),
            vmem((DK, FEATS), bf16),
            vmem((4, COLS, FEATS), bf16),
            vmem((2, RING, COLS, FEATS), bf16),
            vmem((2, RING, PIECES, COLS, FEATS), bf16),
            vmem((LAYERS, FEATS), bf16),
            vmem((LAYERS, COLS), bf16),
            vmem((DP, SEQ, DK), bf16),
            vmem((DP, SEQ, DK), bf16),
            vmem((DP, 1, DK), f32),
            vmem((DP, 1, DK), f32),
            vmem((GROUP, SEQ, DK), bf16),
            vmem((LAYERS, 2, DK), f32),
            vmem((LAYERS, GROUP, 2, DK), f32),
            vmem((DP, 8, DK), bf16),
            vmem((8, DK), bf16),
            vmem((TP, 8, DK), bf16),
            vmem((TP, 8, DK), bf16),
            vmem((8, DK), bf16),
            vmem((TP, 8, DK), bf16),
            vmem((ROWS, DP, ROWS, FEATS), bf16),
            vmem((TP, ROWS, FEATS), bf16),
            dma((15,)),
            dma((4,)),
            dma((4,)),
            dma((3,)),
            dma,
            dma((11,)),
            dma((11,)),
        ],
        compiler_params=pltpu.CompilerParams(collective_id=0, has_side_effects=True),
        name="retention_step",
    )(
        tokens, lengths, states, norm_gain,
        flip(w_query), flip(w_key), flip(w_value), flip(w_gate), head_gain, w_out,
    )


def solution(mesh):
    placed = (
        P("tp", "dp"),
        P("dp"),
        P(None, "dp", "tp", None),
        P(None, "dp"),
        P(None, "dp", "tp"),
        P(None, "dp", "tp"),
        P(None, "dp", "tp"),
        P(None, "dp", "tp"),
        P(None, "tp"),
        P(None, "tp", "dp"),
    )
    return jax.shard_map(
        body,
        mesh=mesh,
        in_specs=placed,
        out_specs=(P("tp", "dp"), P(None, "dp", "tp", None)),
        check_vma=False,
    )
```

```python
import jax
import jax.numpy as jnp
from jax import lax
from jax.experimental import pallas as pl
from jax.experimental.pallas import tpu as pltpu
from jax.sharding import PartitionSpec as P

D = 4096
HEADS = 16
DK = 128
LAYERS = 2
TP = 64
DP = 16
RING = 8
ROWS = 4
FEATS = 256
COLS = 32
SEQ = 16
GROUP = 4
FAR = (4, 5, 3, 6, 2, 7, 1, 0)
PIECES = 11
VALUE, OUT = 8, 10
CUT = 6

norm_eps = 1e-06
group_eps = 1e-05
rotary_base = 10000.0
MESH = pl.DeviceIdType.MESH
f32 = jnp.float32
bf16 = jnp.bfloat16


def hops(a):
    return min(a, RING - a)


PLANE = sorted(
    ((dz, dy) for dz in range(RING) for dy in range(RING) if dz or dy),
    key=lambda o: -(hops(o[0]) + hops(o[1])),
)


def kernel(
    tok, lens, states, ngain, wq, wk, wv, wg, hgain, wout,
    out, st,
    len_s, xo, xg, nrm, wp0, wp1, wo0, w1, ng, hg,
    p2s, p2r, sqs, sqr, pj, stat, stats0, stats1, res_s, res,
    us0, ur0, xb, xg1, us1, ur1, rest_s, rest, means, vsum, vsums,
    lsem, ring_r, ring_l, sib_r, side_s, ss, rs,
):
    tp = lax.axis_index("tp")
    dp = lax.axis_index("dp")
    z, y = lax.div(tp, RING), lax.rem(tp, RING)
    xc, core = lax.div(dp, 2), lax.rem(dp, 2)
    other = 1 - core
    grp, gj = lax.div(tp, GROUP), lax.rem(tp, GROUP)
    z8 = [lax.rem(z + o, RING) * RING for o in range(RING)]
    yo = [lax.rem(y + o, RING) for o in range(RING)]
    xo2 = [lax.rem(xc + o, RING) for o in range(RING)]
    tp_peers = [z8[dz] + yo[dy] for dz, dy in PLANE]
    line = [(o, c) for o in FAR for c in (0, 1) if o or c]
    dp_peers = [xo2[o] * 2 + (other if c else core) for o, c in line]
    group_peers = [grp * GROUP + lax.rem(gj + k, GROUP) for k in (3, 2, 1)]

    load_tok = pltpu.make_async_copy(tok, xo, lsem.at[0])
    load_out = pltpu.make_async_copy(wout.at[0], wo0.at[core, xc], lsem.at[1])
    loads = [
        pltpu.make_async_copy(wq.at[0], wp0.at[0:32], lsem.at[8]),
        pltpu.make_async_copy(wk.at[0], wp0.at[32:64], lsem.at[9]),
        pltpu.make_async_copy(wv.at[0], wp0.at[64:96], lsem.at[10]),
        pltpu.make_async_copy(wg.at[0], wp0.at[96:128], lsem.at[11]),
        pltpu.make_async_copy(wq.at[1], wp1.at[0], lsem.at[2]),
        pltpu.make_async_copy(wk.at[1], wp1.at[1], lsem.at[3]),
        pltpu.make_async_copy(wv.at[1], wp1.at[2], lsem.at[4]),
        pltpu.make_async_copy(wg.at[1], wp1.at[3], lsem.at[5]),
        pltpu.make_async_copy(wout.at[1], w1.at[core, xc, OUT], lsem.at[6]),
        pltpu.make_async_copy(ngain, ng, lsem.at[7]),
        pltpu.make_async_copy(lens, len_s, lsem.at[12]),
        pltpu.make_async_copy(hgain, hg, lsem.at[13]),
        pltpu.make_async_copy(states, st, lsem.at[14]),
    ]
    load_tok.start()
    barrier = pltpu.get_barrier_semaphore()
    for peer in tp_peers:
        pl.semaphore_signal(barrier, inc=1, device_id=(peer, dp), device_id_type=MESH)
    for peer in dp_peers:
        pl.semaphore_signal(barrier, inc=1, device_id=(tp, peer), device_id_type=MESH)
    load_out.start()
    for c in loads:
        c.start()
    load_tok.wait()
    pl.semaphore_wait(barrier, TP + DP - 2)

    sends = []

    def push(src, dst, sem_id, peer_tp, peer_dp):
        pltpu.make_async_remote_copy(
            src_ref=src, dst_ref=dst, send_sem=ss.at[sem_id], recv_sem=rs.at[sem_id],
            device_id=(peer_tp, peer_dp), device_id_type=MESH,
        ).start()

    def push_side(src, dst, recv, peer_dp):
        pltpu.make_async_remote_copy(
            src_ref=src, dst_ref=dst, send_sem=side_s, recv_sem=recv,
            device_id=(tp, peer_dp), device_id_type=MESH,
        ).start()

    def send_group(src, dst, sem_id):
        for peer in group_peers:
            push(src, dst, sem_id, peer, dp)

    def wait_bytes(ref, sem):
        pltpu.make_async_copy(ref, ref, sem).wait()

    def landed(ref, sem_id):
        wait_bytes(ref, rs.at[sem_id])
        sends.append((ref, sem_id))

    right, left, sibling = xo2[1] * 2 + core, xo2[7] * 2 + core, xc * 2 + other

    def ring(step):
        came_right, came_left = xo2[(RING - step) % RING], xo2[step]
        if step == 0:
            landed(w1.at[core, xc, pl.ds(0, 2 * GROUP - 2)], 8)
        elif step < 4:
            wait_bytes(w1.at[core, came_right], ring_r.at[step - 1])
            wait_bytes(w1.at[core, came_left], ring_l.at[step - 1])
        else:
            wait_bytes(w1.at[core, came_right, pl.ds(0, CUT)], ring_r.at[3])
            wait_bytes(w1.at[core, came_left, pl.ds(CUT, PIECES - CUT)], ring_l.at[3])
        if step < 3:
            push_side(w1.at[core, came_right], w1.at[core, came_right], ring_r.at[step], right)
            push_side(w1.at[core, came_left], w1.at[core, came_left], ring_l.at[step], left)
        if step == 3:
            part_r = w1.at[core, came_right, pl.ds(0, CUT)]
            part_l = w1.at[core, came_left, pl.ds(CUT, PIECES - CUT)]
            push_side(part_r, part_r, ring_r.at[3], right)
            push_side(part_l, part_l, ring_l.at[3], left)
        push_side(w1.at[core, came_right], w1.at[core, came_right], sib_r.at[1], sibling)
        if 1 <= step <= 3:
            push_side(w1.at[core, came_left], w1.at[core, came_left], sib_r.at[1], sibling)

    def columns(values_gates):
        both_t = jnp.transpose(jnp.concatenate([values_gates, pad_rows], axis=0))
        values_t, gate_t = both_t[0:COLS, :], both_t[COLS : 2 * COLS, :]
        return values_t, gate_t / (1.0 + jnp.exp(-gate_t))

    def rotated(query, key):
        rq = query * cosine + pltpu.roll(query, half, 1) * sine
        rk = (key * cosine + pltpu.roll(key, half, 1) * sine) * DK ** (-0.5)
        return rq, rk

    def by_sequence(channels_t):
        full = jnp.concatenate([channels_t, jnp.zeros((DK - COLS, DK), f32)], axis=0)
        return jnp.transpose(full)[0:SEQ, 0:COLS].astype(bf16)

    def readout(rq, rk, values_t, value_mean, l):
        read = jnp.zeros((COLS, DK), f32)
        for s in range(SEQ):
            r = jnp.sum(st[l, s] * rq[s : s + 1, :], axis=1, keepdims=True)
            read = jnp.where(lane32 == s, r, read)
        match = jnp.sum(rq * rk, axis=1, keepdims=True)
        state_mean = (means[0, l] + means[1, l]) + (means[2, l] + means[3, l])
        mean_v = jnp.sum(rq * state_mean, axis=1, keepdims=True) * gamma[0:SEQ, 0:1]
        mean_v = mean_v + match * value_mean
        match = jnp.sum(jnp.where(diag, match, 0.0), axis=0, keepdims=True)
        mean_v = jnp.sum(jnp.where(diag, mean_v, 0.0), axis=0, keepdims=True)
        read = gamma * read + values_t * match - mean_v
        stat[l] = jnp.sum(read * read, axis=0, keepdims=True)
        return read

    def update(rk, values_t, l):
        for s in range(SEQ):
            st[l, s] = gamma * st[l, s] + values_t[:, s : s + 1] * rk[s : s + 1, :]

    t_row = lax.broadcasted_iota(jnp.int32, (TP, DK), 0)

    def coefficients(ref):
        head_sum = ref[...].reshape(TP, DK)
        for bit in (1, 2):
            up = lax.rem(lax.div(t_row, bit), 2) == 1
            head_sum = head_sum + jnp.where(
                up, pltpu.roll(head_sum, bit, 0), pltpu.roll(head_sum, TP - bit, 0)
            )
        scale = lax.rsqrt(head_sum / DK + group_eps)
        return jnp.transpose(jnp.concatenate([scale, scale], axis=0))

    def scaled(coef, ref):
        acc = None
        for g in range(0, TP, GROUP):
            part = [ref[g + j].astype(f32) for j in range(GROUP)]
            part = coef[:, g : g + 1] * ((part[0] + part[1]) + (part[2] + part[3]))
            acc = part if acc is None else acc + part
        return acc

    for peer in tp_peers:
        push(xo, xg.at[tp], 0, peer, dp)
    xg[tp] = xo[...]
    load_out.wait()
    for o in FAR[:7]:
        push_side(wo0.at[core, xc], wo0.at[core, xc], sib_r.at[2], xo2[o] * 2 + core)
    for c in loads:
        c.wait()
    row = lax.broadcasted_iota(jnp.int32, (SEQ, DK), 0)
    lane = lax.broadcasted_iota(jnp.int32, (SEQ, DK), 1)
    diag = row == lane
    lane32 = lax.broadcasted_iota(jnp.int32, (COLS, DK), 1)
    row32 = lax.broadcasted_iota(jnp.int32, (COLS, COLS), 0)
    col32 = lax.broadcasted_iota(jnp.int32, (COLS, COLS), 1)
    pos = jnp.zeros((SEQ, DK), jnp.int32)
    for s in range(SEQ):
        pos = jnp.where(row == s, len_s[s], pos)
    half = DK // 2
    exponent = lax.rem(lane, half).astype(f32) / half
    inverse = jnp.exp(exponent * (-9.210340371976184))
    angle = pos.astype(f32) * inverse
    cosine = jnp.cos(angle)
    sine = jnp.sin(angle)
    sine = jnp.where(lane < half, -sine, sine)
    head = (jnp.zeros((COLS, DK), jnp.int32) + grp).astype(f32)
    gamma = 1.0 - jnp.exp2(-1.0 - 9.0 * head / (HEADS - 1))
    hgains = [
        jnp.sum(jnp.where(row32 == col32, hg[l : l + 1, :].astype(f32), 0.0), axis=1, keepdims=True)
        for l in range(LAYERS)
    ]
    pad_rows = jnp.zeros((DK - SEQ, DK), f32)
    gain = ng[1:2, :].astype(f32)
    for piece, n in ((gj, 0), (GROUP + gj, 1), (VALUE, 2), (VALUE + 1, 3)):
        w1[core, xc, piece] = (wp1[n].astype(f32) * gain).astype(bf16)
    vsum[gj] = jnp.sum(w1[core, xc, VALUE].astype(f32), axis=0, keepdims=True)
    for l in range(LAYERS):
        means[gj, l] = jnp.sum(st[l], axis=1) / DK
    send_group(vsum.at[gj], vsum.at[gj], 5)
    for piece in (gj, GROUP + gj):
        send_group(w1.at[core, xc, piece], w1.at[core, xc, piece], 8)
    landed(xg.at[pl.ds(0, TP - 1)], 0)
    gain = ng[0:1, :].astype(f32)
    res_half, res_side = lax.div(tp, 32), lax.rem(tp, 2)
    for d in range(DP):
        xf = jnp.concatenate([xg[4 * d + j].astype(f32) for j in range(4)], axis=0)
        squares = jnp.sum(xf * xf, axis=1, keepdims=True)
        sqs[d] = jnp.sum(jnp.where(diag, squares, 0.0), axis=0, keepdims=True)
        nrm[pl.ds(SEQ * d, SEQ), :] = (xf * gain).astype(bf16)
        part8 = jnp.where(res_half == 1, xf[8:16], xf[0:8])
        res_s[d] = jnp.where(res_side == 1, part8[:, DK:], part8[:, :DK]).astype(bf16)
    part = lax.dot_general(
        nrm[...], wp0[...], (((1,), (1,)), ((), ())), preferred_element_type=f32
    )
    p2s[...] = part.astype(bf16).reshape(DP, SEQ, DK)
    for peer in dp_peers:
        push(p2s.at[peer], p2r.at[dp], 1, tp, peer)
        push(sqs.at[peer], sqr.at[dp], 2, tp, peer)
    send_group(means.at[gj], means.at[gj], 9)
    p2r[dp] = p2s[dp]
    sqr[dp] = sqs[dp]
    res_owner = lax.rem(lax.div(tp, 2), DP)

    @pl.when(dp == res_owner)
    def _():
        for peer in dp_peers:
            push(res_s.at[peer], res, 3, tp, peer)
        res[...] = res_s[dp]

    wait_bytes(wo0.at[core, pl.ds(0, RING - 1)], sib_r.at[2])
    push_side(wo0.at[core], wo0.at[core], sib_r.at[0], sibling)
    ring(0)
    landed(vsum.at[pl.ds(0, GROUP - 1)], 5)
    vsums[dp] = (vsum[0] + vsum[1]) + (vsum[2] + vsum[3])
    for peer in dp_peers:
        push(vsums.at[dp], vsums.at[dp], 14, tp, peer)
    landed(p2r.at[pl.ds(0, DP - 1)], 1)
    landed(sqr.at[pl.ds(0, DP - 1)], 2)
    total = jnp.sum(p2r[...].astype(f32), axis=0)
    squares = jnp.sum(sqr[...], axis=0)
    squares = jnp.sum(jnp.where(diag, squares, 0.0), axis=1, keepdims=True)
    proj = (total * lax.rsqrt(squares / D + norm_eps)).astype(bf16)

    pj[gj] = proj
    send_group(pj.at[gj], pj.at[gj], 4)
    values_t, silu_t = columns(pltpu.roll(proj.astype(f32), 2 * COLS, 1))
    wait_bytes(wo0.at[other], sib_r.at[0])

    def first_blocks(left_side, ref):
        for d in range(DP):
            term = jnp.dot(left_side, wo0[d % 2, d // 2], preferred_element_type=f32)
            for h in range(2):
                for k in range(2):
                    ref[32 * h + 2 * d + k] = term[
                        8 * h : 8 * h + 8, DK * k : DK * k + DK
                    ].astype(bf16)

    weight_t = silu_t * hgains[0]
    ring(1)
    landed(means.at[pl.ds(0, GROUP - 1)], 9)
    landed(pj.at[pl.ds(0, GROUP - 1)], 4)
    value_mean = jnp.zeros((SEQ, DK), f32)
    query = jnp.zeros((SEQ, DK), f32)
    key = jnp.zeros((SEQ, DK), f32)
    for j in range(GROUP):
        piece = pj[j].astype(f32)
        value_mean = value_mean + piece
        here = lax.div(lane, COLS) == j
        query = jnp.where(here, pltpu.roll(piece, COLS * j, 1) if j else piece, query)
        shift = (COLS * j - COLS) % DK
        key = jnp.where(here, pltpu.roll(piece, shift, 1) if shift else piece, key)
    rq, rk = rotated(query, key)
    is_value = lax.div(lane, COLS) == 2
    value_mean = jnp.sum(jnp.where(is_value, value_mean, 0.0), axis=1, keepdims=True) / DK
    read = readout(rq, rk, values_t, value_mean, 0)
    for peer in tp_peers:
        push(stat.at[0], stats0.at[tp], 11, peer, dp)
    first_blocks(by_sequence(weight_t * read), us0)
    for peer in tp_peers:
        push(us0.at[peer], ur0.at[tp], 6, peer, dp)
    stats0[tp] = stat[0]
    ur0[tp] = us0[tp]
    update(rk, values_t, 0)
    ring(2)
    landed(stats0.at[pl.ds(0, TP - 1)], 11)
    coef = coefficients(stats0)
    coef = jnp.where(res_half == 1, coef[8:16], coef[0:8])
    @pl.when(dp != res_owner)
    def _():
        wait_bytes(res, rs.at[3])

    base = res[...].astype(f32)
    landed(ur0.at[pl.ds(0, TP - 1)], 6)
    xb[...] = (base + scaled(coef, ur0)).astype(bf16)

    for peer in tp_peers:
        push(xb, xg1.at[tp], 7, peer, dp)
    xg1[tp] = xb[...]
    ring(3)
    ring(4)
    landed(xg1.at[pl.ds(0, TP - 1)], 7)

    def features(d):
        halves = [
            jnp.concatenate([xg1[32 * h + 2 * d + k].astype(f32) for k in range(2)], axis=1)
            for h in range(2)
        ]
        return jnp.concatenate(halves, axis=0)

    rest_j, rest_d = lax.div(tp, DP), lax.rem(tp, DP)
    rest_tp = ROWS * dp + rest_j
    rest_at = 32 * lax.div(rest_j, 2) + 2 * rest_d
    piece = jnp.concatenate([xg1[rest_at + k].astype(f32) for k in range(2)], axis=1)
    rest_s[...] = jnp.where(lax.rem(rest_j, 2) == 1, piece[4:8], piece[0:4]).astype(bf16)
    rest_here = jnp.logical_and(tp == rest_tp, dp == rest_d)

    @pl.when(rest_here)
    def _():
        pltpu.make_async_copy(rest_s, rest, rs.at[13]).start()

    @pl.when(jnp.logical_not(rest_here))
    def _():
        push(rest_s, rest, 13, rest_tp, rest_d)

    squares = jnp.zeros((SEQ, FEATS), f32)
    total = jnp.zeros((SEQ, COLS * OUT), f32)
    value_sum = jnp.zeros((SEQ, FEATS), f32)
    landed(vsums.at[pl.ds(0, DP - 1)], 14)
    for c in (core, other):
        if c is other:
            wait_bytes(w1.at[other], sib_r.at[1])
        for o in range(RING):
            xf = features(2 * o + c)
            squares = squares + xf * xf
            value_sum = value_sum + xf * vsums[2 * o + c]
            total = total + lax.dot_general(
                xf.astype(bf16), w1[c, o, 0:OUT].reshape(COLS * OUT, FEATS),
                (((1,), (1,)), ((), ())), preferred_element_type=f32,
            )
    squares = jnp.sum(squares, axis=1, keepdims=True)
    row_scale = lax.rsqrt(squares / D + norm_eps)
    value_mean = jnp.sum(value_sum, axis=1, keepdims=True) * row_scale / DK
    proj = (total * row_scale).astype(bf16).astype(f32)
    rq, rk = rotated(proj[:, 0:DK], proj[:, DK : 2 * DK])
    tail = jnp.concatenate([proj[:, 2 * DK :], jnp.zeros((SEQ, DK - 2 * COLS), f32)], axis=1)
    values_t, silu_t = columns(tail)

    def last_blocks(left_side, ref):
        for d in range(DP):
            term = jnp.dot(left_side, w1[d % 2, d // 2, OUT], preferred_element_type=f32)
            for j in range(ROWS):
                ref[j, d] = term[ROWS * j : ROWS * j + ROWS].astype(bf16)

    def push_last(src_of, dst, sem_id):
        for peer in dp_peers:
            for j in range(ROWS):
                push(src_of(j, peer), dst, sem_id, ROWS * dp + j, peer)
        for j in range(ROWS):
            here = tp == ROWS * dp + j

            @pl.when(here)
            def _():
                pltpu.make_async_copy(src_of(j, dp), dst, rs.at[sem_id]).start()

            @pl.when(jnp.logical_not(here))
            def _():
                push(src_of(j, dp), dst, sem_id, ROWS * dp + j, dp)

    weight_t = silu_t * hgains[1]
    read = readout(rq, rk, values_t, value_mean, 1)
    push_last(lambda j, peer: stat.at[1], stats1.at[tp], 12)
    last_blocks(by_sequence(weight_t * read), us1)
    push_last(lambda j, peer: us1.at[j, peer], ur1.at[tp], 10)
    update(rk, values_t, 1)
    wait_bytes(stats1, rs.at[12])
    coef = coefficients(stats1)
    coef = jnp.where(
        gj < 2,
        jnp.where(gj == 0, coef[0:4], coef[4:8]),
        jnp.where(gj == 2, coef[8:12], coef[12:16]),
    )
    wait_bytes(rest, rs.at[13])
    base = rest[...].astype(f32)
    wait_bytes(ur1, rs.at[10])
    out[...] = (base + scaled(coef, ur1)).astype(bf16)

    for ref, sem_id in sends:
        wait_bytes(ref, ss.at[sem_id])

    @pl.when(dp == res_owner)
    def _():
        wait_bytes(res_s.at[pl.ds(0, DP - 1)], ss.at[3])

    last = ((ur1, 10), (stats1, 12))

    @pl.when(lax.div(tp, ROWS) == dp)
    def _():
        for ref, sem_id in last:
            wait_bytes(ref.at[pl.ds(0, TP - 1)], ss.at[sem_id])

    @pl.when(lax.div(tp, ROWS) != dp)
    def _():
        for ref, sem_id in last:
            wait_bytes(ref, ss.at[sem_id])

    @pl.when(jnp.logical_not(rest_here))
    def _():
        wait_bytes(rest, ss.at[13])

    wait_bytes(wo0.at[0, pl.ds(0, RING - 1)], side_s)
    wait_bytes(wo0.at[0], side_s)
    wait_bytes(w1.at[0, pl.ds(0, RING - 1)], side_s)
    wait_bytes(w1.at[0], side_s)


def body(tokens, lengths, states, norm_gain, w_query, w_key, w_value, w_gate, head_gain, w_out):
    flip = lambda w: jnp.transpose(w, (0, 2, 1))
    hbm = pl.BlockSpec(memory_space=pl.ANY)
    vmem = pltpu.VMEM
    dma = pltpu.SemaphoreType.DMA
    return pl.pallas_call(
        kernel,
        out_shape=(vmem((ROWS, FEATS), bf16), vmem(states.shape, f32)),
        in_specs=[hbm] * 10,
        out_specs=(pl.BlockSpec(memory_space=vmem), pl.BlockSpec(memory_space=vmem)),
        scratch_shapes=[
            pltpu.SMEM((SEQ,), jnp.int32),
            vmem((ROWS, FEATS), bf16),
            vmem((TP, ROWS, FEATS), bf16),
            vmem((TP * ROWS, FEATS), bf16),
            vmem((DK, FEATS), bf16),
            vmem((4, COLS, FEATS), bf16),
            vmem((2, RING, COLS, FEATS), bf16),
            vmem((2, RING, PIECES, COLS, FEATS), bf16),
            vmem((LAYERS, FEATS), bf16),
            vmem((LAYERS, COLS), bf16),
            vmem((DP, SEQ, DK), bf16),
            vmem((DP, SEQ, DK), bf16),
            vmem((DP, 1, DK), f32),
            vmem((DP, 1, DK), f32),
            vmem((GROUP, SEQ, DK), bf16),
            vmem((LAYERS, 1, DK), f32),
            vmem((TP, 1, DK), f32),
            vmem((TP, 1, DK), f32),
            vmem((DP, 8, DK), bf16),
            vmem((8, DK), bf16),
            vmem((TP, 8, DK), bf16),
            vmem((TP, 8, DK), bf16),
            vmem((8, DK), bf16),
            vmem((TP, 8, DK), bf16),
            vmem((ROWS, DP, ROWS, FEATS), bf16),
            vmem((TP, ROWS, FEATS), bf16),
            vmem((ROWS, FEATS), bf16),
            vmem((ROWS, FEATS), bf16),
            vmem((GROUP, LAYERS, SEQ, DK), f32),
            vmem((GROUP, 1, FEATS), f32),
            vmem((DP, 1, FEATS), f32),
            dma((15,)),
            dma((4,)),
            dma((4,)),
            dma((3,)),
            dma,
            dma((15,)),
            dma((15,)),
        ],
        compiler_params=pltpu.CompilerParams(collective_id=0, has_side_effects=True),
        name="retention_step",
    )(
        tokens, lengths, states, norm_gain,
        flip(w_query), flip(w_key), flip(w_value), flip(w_gate), head_gain, w_out,
    )


def solution(mesh):
    placed = (
        P("tp", "dp"),
        P("dp"),
        P(None, "dp", "tp", None),
        P(None, "dp"),
        P(None, "dp", "tp"),
        P(None, "dp", "tp"),
        P(None, "dp", "tp"),
        P(None, "dp", "tp"),
        P(None, "tp"),
        P(None, "tp", "dp"),
    )
    return jax.shard_map(
        body,
        mesh=mesh,
        in_specs=placed,
        out_specs=(P("tp", "dp"), P(None, "dp", "tp", None)),
        check_vma=False,
    )
```

```python
import jax
import jax.numpy as jnp
from jax import lax
from jax.experimental import pallas as pl
from jax.experimental.pallas import tpu as pltpu
from jax.sharding import PartitionSpec as P

D = 4096
HEADS = 16
DK = 128
LAYERS = 2
TP = 64
DP = 16
RING = 8
ROWS = 4
FEATS = 256
COLS = 32
SEQ = 16
GROUP = 4
FAR = (4, 5, 3, 6, 2, 7, 1, 0)
PIECES = 11
VALUE, OUT = 8, 10
CUT = 6

norm_eps = 1e-06
group_eps = 1e-05
rotary_base = 10000.0
MESH = pl.DeviceIdType.MESH
f32 = jnp.float32
bf16 = jnp.bfloat16


def hops(a):
    return min(a, RING - a)


PLANE = sorted(
    ((dz, dy) for dz in range(RING) for dy in range(RING) if dz or dy),
    key=lambda o: -(hops(o[0]) + hops(o[1])),
)


def kernel(
    tok, lens, states, ngain, wq, wk, wv, wg, hgain, wout,
    out, st,
    len_s, xo, xg, nrm, wp0, wp1, wo0, w1, ng, hg,
    p2s, p2r, sqs, sqr, pj, stat, stats0, stats1, res_s, res,
    us0, ur0, xb, xg1, us1, ur1, rest_s, rest, means, vsum, vsums,
    lsem, ring_r, ring_l, sib_r, side_s, ss, rs,
):
    tp = lax.axis_index("tp")
    dp = lax.axis_index("dp")
    z, y = lax.div(tp, RING), lax.rem(tp, RING)
    xc, core = lax.div(dp, 2), lax.rem(dp, 2)
    other = 1 - core
    grp, gj = lax.div(tp, GROUP), lax.rem(tp, GROUP)
    z8 = [lax.rem(z + o, RING) * RING for o in range(RING)]
    yo = [lax.rem(y + o, RING) for o in range(RING)]
    xo2 = [lax.rem(xc + o, RING) for o in range(RING)]
    tp_peers = [z8[dz] + yo[dy] for dz, dy in PLANE]
    line = [(o, c) for o in FAR for c in (0, 1) if o or c]
    dp_peers = [xo2[o] * 2 + (other if c else core) for o, c in line]
    group_peers = [grp * GROUP + lax.rem(gj + k, GROUP) for k in (3, 2, 1)]

    load_tok = pltpu.make_async_copy(tok, xo, lsem.at[0])
    load_out = pltpu.make_async_copy(wout.at[0], wo0.at[core, xc], lsem.at[1])
    loads = [
        pltpu.make_async_copy(wq.at[0], wp0.at[0:32], lsem.at[8]),
        pltpu.make_async_copy(wk.at[0], wp0.at[32:64], lsem.at[9]),
        pltpu.make_async_copy(wv.at[0], wp0.at[64:96], lsem.at[10]),
        pltpu.make_async_copy(wg.at[0], wp0.at[96:128], lsem.at[11]),
        pltpu.make_async_copy(wq.at[1], wp1.at[0], lsem.at[2]),
        pltpu.make_async_copy(wk.at[1], wp1.at[1], lsem.at[3]),
        pltpu.make_async_copy(wv.at[1], wp1.at[2], lsem.at[4]),
        pltpu.make_async_copy(wg.at[1], wp1.at[3], lsem.at[5]),
        pltpu.make_async_copy(wout.at[1], w1.at[core, xc, OUT], lsem.at[6]),
        pltpu.make_async_copy(ngain, ng, lsem.at[7]),
        pltpu.make_async_copy(lens, len_s, lsem.at[12]),
        pltpu.make_async_copy(hgain, hg, lsem.at[13]),
        pltpu.make_async_copy(states, st, lsem.at[14]),
    ]
    load_tok.start()
    barrier = pltpu.get_barrier_semaphore()
    for peer in tp_peers:
        pl.semaphore_signal(barrier, inc=1, device_id=(peer, dp), device_id_type=MESH)
    for peer in dp_peers:
        pl.semaphore_signal(barrier, inc=1, device_id=(tp, peer), device_id_type=MESH)
    load_out.start()
    for c in loads:
        c.start()
    load_tok.wait()
    pl.semaphore_wait(barrier, TP + DP - 2)

    sends = []

    def push(src, dst, sem_id, peer_tp, peer_dp):
        pltpu.make_async_remote_copy(
            src_ref=src, dst_ref=dst, send_sem=ss.at[sem_id], recv_sem=rs.at[sem_id],
            device_id=(peer_tp, peer_dp), device_id_type=MESH,
        ).start()

    def push_side(src, dst, recv, peer_dp):
        pltpu.make_async_remote_copy(
            src_ref=src, dst_ref=dst, send_sem=side_s, recv_sem=recv,
            device_id=(tp, peer_dp), device_id_type=MESH,
        ).start()

    def send_group(src, dst, sem_id):
        for peer in group_peers:
            push(src, dst, sem_id, peer, dp)

    def wait_bytes(ref, sem):
        pltpu.make_async_copy(ref, ref, sem).wait()

    def landed(ref, sem_id):
        wait_bytes(ref, rs.at[sem_id])
        sends.append((ref, sem_id))

    right, left, sibling = xo2[1] * 2 + core, xo2[7] * 2 + core, xc * 2 + other

    def ring(step):
        came_right, came_left = xo2[(RING - step) % RING], xo2[step]
        if step == 0:
            landed(w1.at[core, xc, pl.ds(0, 2 * GROUP - 2)], 8)
        elif step < 4:
            wait_bytes(w1.at[core, came_right], ring_r.at[step - 1])
            wait_bytes(w1.at[core, came_left], ring_l.at[step - 1])
        else:
            wait_bytes(w1.at[core, came_right, pl.ds(0, CUT)], ring_r.at[3])
            wait_bytes(w1.at[core, came_left, pl.ds(CUT, PIECES - CUT)], ring_l.at[3])
        if step < 3:
            push_side(w1.at[core, came_right], w1.at[core, came_right], ring_r.at[step], right)
            push_side(w1.at[core, came_left], w1.at[core, came_left], ring_l.at[step], left)
        if step == 3:
            part_r = w1.at[core, came_right, pl.ds(0, CUT)]
            part_l = w1.at[core, came_left, pl.ds(CUT, PIECES - CUT)]
            push_side(part_r, part_r, ring_r.at[3], right)
            push_side(part_l, part_l, ring_l.at[3], left)
        push_side(w1.at[core, came_right], w1.at[core, came_right], sib_r.at[1], sibling)
        if 1 <= step <= 3:
            push_side(w1.at[core, came_left], w1.at[core, came_left], sib_r.at[1], sibling)

    def columns(values_gates):
        both_t = jnp.transpose(jnp.concatenate([values_gates, pad_rows], axis=0))
        values_t, gate_t = both_t[0:COLS, :], both_t[COLS : 2 * COLS, :]
        return values_t, gate_t / (1.0 + jnp.exp(-gate_t))

    def rotated(query, key):
        rq = query * cosine + pltpu.roll(query, half, 1) * sine
        rk = (key * cosine + pltpu.roll(key, half, 1) * sine) * DK ** (-0.5)
        return rq, rk

    def by_sequence(channels_t):
        full = jnp.concatenate([channels_t, jnp.zeros((DK - COLS, DK), f32)], axis=0)
        return jnp.transpose(full)[0:SEQ, 0:COLS].astype(bf16)

    def readout(rq, rk, values_t, value_mean, l):
        read = jnp.zeros((COLS, DK), f32)
        for s in range(SEQ):
            r = jnp.sum(st[l, s] * rq[s : s + 1, :], axis=1, keepdims=True)
            read = jnp.where(lane32 == s, r, read)
        match = jnp.sum(rq * rk, axis=1, keepdims=True)
        state_mean = (means[0, l] + means[1, l]) + (means[2, l] + means[3, l])
        mean_v = jnp.sum(rq * state_mean, axis=1, keepdims=True) * gamma[0:SEQ, 0:1]
        mean_v = mean_v + match * value_mean
        match = jnp.sum(jnp.where(diag, match, 0.0), axis=0, keepdims=True)
        mean_v = jnp.sum(jnp.where(diag, mean_v, 0.0), axis=0, keepdims=True)
        read = gamma * read + values_t * match - mean_v
        stat[l] = jnp.sum(read * read, axis=0, keepdims=True)
        return read

    def update(rk, values_t, l):
        for s in range(SEQ):
            st[l, s] = gamma * st[l, s] + values_t[:, s : s + 1] * rk[s : s + 1, :]

    t_row = lax.broadcasted_iota(jnp.int32, (TP, DK), 0)

    def coefficients(ref):
        head_sum = ref[...].reshape(TP, DK)
        for bit in (1, 2):
            up = lax.rem(lax.div(t_row, bit), 2) == 1
            head_sum = head_sum + jnp.where(
                up, pltpu.roll(head_sum, bit, 0), pltpu.roll(head_sum, TP - bit, 0)
            )
        scale = lax.rsqrt(head_sum / DK + group_eps)
        return jnp.transpose(jnp.concatenate([scale, scale], axis=0))

    def scaled(coef, ref):
        acc = None
        for g in range(0, TP, GROUP):
            part = [ref[g + j].astype(f32) for j in range(GROUP)]
            part = coef[:, g : g + 1] * ((part[0] + part[1]) + (part[2] + part[3]))
            acc = part if acc is None else acc + part
        return acc

    for peer in tp_peers:
        push(xo, xg.at[tp], 0, peer, dp)
    xg[tp] = xo[...]
    load_out.wait()
    for o in FAR[:7]:
        push_side(wo0.at[core, xc], wo0.at[core, xc], sib_r.at[2], xo2[o] * 2 + core)
    for c in loads:
        c.wait()
    row = lax.broadcasted_iota(jnp.int32, (SEQ, DK), 0)
    lane = lax.broadcasted_iota(jnp.int32, (SEQ, DK), 1)
    diag = row == lane
    lane32 = lax.broadcasted_iota(jnp.int32, (COLS, DK), 1)
    row32 = lax.broadcasted_iota(jnp.int32, (COLS, COLS), 0)
    col32 = lax.broadcasted_iota(jnp.int32, (COLS, COLS), 1)
    pos = jnp.zeros((SEQ, DK), jnp.int32)
    for s in range(SEQ):
        pos = jnp.where(row == s, len_s[s], pos)
    half = DK // 2
    exponent = lax.rem(lane, half).astype(f32) / half
    inverse = jnp.exp(exponent * (-9.210340371976184))
    angle = pos.astype(f32) * inverse
    cosine = jnp.cos(angle)
    sine = jnp.sin(angle)
    sine = jnp.where(lane < half, -sine, sine)
    head = (jnp.zeros((COLS, DK), jnp.int32) + grp).astype(f32)
    gamma = 1.0 - jnp.exp2(-1.0 - 9.0 * head / (HEADS - 1))
    hgains = [
        jnp.sum(jnp.where(row32 == col32, hg[l : l + 1, :].astype(f32), 0.0), axis=1, keepdims=True)
        for l in range(LAYERS)
    ]
    pad_rows = jnp.zeros((DK - SEQ, DK), f32)
    gain = ng[1:2, :].astype(f32)
    for piece, n in ((gj, 0), (GROUP + gj, 1), (VALUE, 2), (VALUE + 1, 3)):
        w1[core, xc, piece] = (wp1[n].astype(f32) * gain).astype(bf16)
    vsum[gj] = jnp.sum(w1[core, xc, VALUE].astype(f32), axis=0, keepdims=True)
    for l in range(LAYERS):
        means[gj, l] = jnp.sum(st[l], axis=1) / DK
    send_group(vsum.at[gj], vsum.at[gj], 5)
    for piece in (gj, GROUP + gj):
        send_group(w1.at[core, xc, piece], w1.at[core, xc, piece], 8)
    landed(xg.at[pl.ds(0, TP - 1)], 0)
    gain = ng[0:1, :].astype(f32)
    res_half, res_side = lax.div(tp, 32), lax.rem(tp, 2)
    for d in range(DP):
        xf = jnp.concatenate([xg[4 * d + j].astype(f32) for j in range(4)], axis=0)
        squares = jnp.sum(xf * xf, axis=1, keepdims=True)
        sqs[d] = jnp.sum(jnp.where(diag, squares, 0.0), axis=0, keepdims=True)
        nrm[pl.ds(SEQ * d, SEQ), :] = (xf * gain).astype(bf16)
        part8 = jnp.where(res_half == 1, xf[8:16], xf[0:8])
        res_s[d] = jnp.where(res_side == 1, part8[:, DK:], part8[:, :DK]).astype(bf16)
    part = lax.dot_general(
        nrm[...], wp0[...], (((1,), (1,)), ((), ())), preferred_element_type=f32
    )
    p2s[...] = part.astype(bf16).reshape(DP, SEQ, DK)
    for peer in dp_peers:
        push(p2s.at[peer], p2r.at[dp], 1, tp, peer)
        push(sqs.at[peer], sqr.at[dp], 2, tp, peer)
    send_group(means.at[gj], means.at[gj], 9)
    p2r[dp] = p2s[dp]
    sqr[dp] = sqs[dp]
    res_owner = lax.rem(lax.div(tp, 2), DP)

    @pl.when(dp == res_owner)
    def _():
        for peer in dp_peers:
            push(res_s.at[peer], res, 3, tp, peer)
        res[...] = res_s[dp]

    wait_bytes(wo0.at[core, pl.ds(0, RING - 1)], sib_r.at[2])
    push_side(wo0.at[core], wo0.at[core], sib_r.at[0], sibling)
    ring(0)
    landed(vsum.at[pl.ds(0, GROUP - 1)], 5)
    vsums[dp] = (vsum[0] + vsum[1]) + (vsum[2] + vsum[3])
    for peer in dp_peers:
        push(vsums.at[dp], vsums.at[dp], 14, tp, peer)
    landed(p2r.at[pl.ds(0, DP - 1)], 1)
    landed(sqr.at[pl.ds(0, DP - 1)], 2)
    total = jnp.sum(p2r[...].astype(f32), axis=0)
    squares = jnp.sum(sqr[...], axis=0)
    squares = jnp.sum(jnp.where(diag, squares, 0.0), axis=1, keepdims=True)
    proj = (total * lax.rsqrt(squares / D + norm_eps)).astype(bf16)

    pj[gj] = proj
    send_group(pj.at[gj], pj.at[gj], 4)
    values_t, silu_t = columns(pltpu.roll(proj.astype(f32), 2 * COLS, 1))
    wait_bytes(wo0.at[other], sib_r.at[0])

    def first_blocks(left_side, ref):
        for d in range(DP):
            term = jnp.dot(left_side, wo0[d % 2, d // 2], preferred_element_type=f32)
            for h in range(2):
                for k in range(2):
                    ref[32 * h + 2 * d + k] = term[
                        8 * h : 8 * h + 8, DK * k : DK * k + DK
                    ].astype(bf16)

    weight_t = silu_t * hgains[0]
    ring(1)
    landed(means.at[pl.ds(0, GROUP - 1)], 9)
    landed(pj.at[pl.ds(0, GROUP - 1)], 4)
    value_mean = jnp.zeros((SEQ, DK), f32)
    query = jnp.zeros((SEQ, DK), f32)
    key = jnp.zeros((SEQ, DK), f32)
    for j in range(GROUP):
        piece = pj[j].astype(f32)
        value_mean = value_mean + piece
        here = lax.div(lane, COLS) == j
        query = jnp.where(here, pltpu.roll(piece, COLS * j, 1) if j else piece, query)
        shift = (COLS * j - COLS) % DK
        key = jnp.where(here, pltpu.roll(piece, shift, 1) if shift else piece, key)
    rq, rk = rotated(query, key)
    is_value = lax.div(lane, COLS) == 2
    value_mean = jnp.sum(jnp.where(is_value, value_mean, 0.0), axis=1, keepdims=True) / DK
    read = readout(rq, rk, values_t, value_mean, 0)
    for peer in tp_peers:
        push(stat.at[0], stats0.at[tp], 11, peer, dp)
    first_blocks(by_sequence(weight_t * read), us0)
    for peer in tp_peers:
        push(us0.at[peer], ur0.at[tp], 6, peer, dp)
    stats0[tp] = stat[0]
    ur0[tp] = us0[tp]
    update(rk, values_t, 0)
    ring(2)
    landed(stats0.at[pl.ds(0, TP - 1)], 11)
    coef = coefficients(stats0)
    coef = jnp.where(res_half == 1, coef[8:16], coef[0:8])
    @pl.when(dp != res_owner)
    def _():
        wait_bytes(res, rs.at[3])

    base = res[...].astype(f32)
    landed(ur0.at[pl.ds(0, TP - 1)], 6)
    xb[...] = (base + scaled(coef, ur0)).astype(bf16)

    for peer in tp_peers:
        push(xb, xg1.at[tp], 7, peer, dp)
    xg1[tp] = xb[...]
    ring(3)
    ring(4)
    landed(xg1.at[pl.ds(0, TP - 1)], 7)

    def features(d):
        halves = [
            jnp.concatenate([xg1[32 * h + 2 * d + k].astype(f32) for k in range(2)], axis=1)
            for h in range(2)
        ]
        return jnp.concatenate(halves, axis=0)

    rest_j, rest_d = lax.div(tp, DP), lax.rem(tp, DP)
    rest_tp = ROWS * dp + rest_j
    rest_at = 32 * lax.div(rest_j, 2) + 2 * rest_d
    piece = jnp.concatenate([xg1[rest_at + k].astype(f32) for k in range(2)], axis=1)
    rest_s[...] = jnp.where(lax.rem(rest_j, 2) == 1, piece[4:8], piece[0:4]).astype(bf16)
    rest_here = jnp.logical_and(tp == rest_tp, dp == rest_d)

    @pl.when(rest_here)
    def _():
        pltpu.make_async_copy(rest_s, rest, rs.at[13]).start()

    @pl.when(jnp.logical_not(rest_here))
    def _():
        push(rest_s, rest, 13, rest_tp, rest_d)

    squares = jnp.zeros((SEQ, FEATS), f32)
    total = jnp.zeros((SEQ, COLS * OUT), f32)
    value_sum = jnp.zeros((SEQ, FEATS), f32)
    landed(vsums.at[pl.ds(0, DP - 1)], 14)
    for c in (core, other):
        if c is other:
            wait_bytes(w1.at[other], sib_r.at[1])
        for o in range(RING):
            xf = features(2 * o + c)
            squares = squares + xf * xf
            value_sum = value_sum + xf * vsums[2 * o + c]
            total = total + lax.dot_general(
                xf.astype(bf16), w1[c, o, 0:OUT].reshape(COLS * OUT, FEATS),
                (((1,), (1,)), ((), ())), preferred_element_type=f32,
            )
    squares = jnp.sum(squares, axis=1, keepdims=True)
    row_scale = lax.rsqrt(squares / D + norm_eps)
    value_mean = jnp.sum(value_sum, axis=1, keepdims=True) * row_scale / DK
    proj = (total * row_scale).astype(bf16).astype(f32)
    rq, rk = rotated(proj[:, 0:DK], proj[:, DK : 2 * DK])
    tail = jnp.concatenate([proj[:, 2 * DK :], jnp.zeros((SEQ, DK - 2 * COLS), f32)], axis=1)
    values_t, silu_t = columns(tail)

    def last_blocks(left_side, ref):
        for d in range(DP):
            term = jnp.dot(left_side, w1[d % 2, d // 2, OUT], preferred_element_type=f32)
            for j in range(ROWS):
                ref[j, d] = term[ROWS * j : ROWS * j + ROWS].astype(bf16)

    def push_last(src_of, dst, sem_id):
        for peer in dp_peers[::-1]:
            for j in range(ROWS):
                push(src_of(j, peer), dst, sem_id, ROWS * dp + j, peer)
        for j in range(ROWS):
            here = tp == ROWS * dp + j

            @pl.when(here)
            def _():
                pltpu.make_async_copy(src_of(j, dp), dst, rs.at[sem_id]).start()

            @pl.when(jnp.logical_not(here))
            def _():
                push(src_of(j, dp), dst, sem_id, ROWS * dp + j, dp)

    weight_t = silu_t * hgains[1]
    read = readout(rq, rk, values_t, value_mean, 1)
    push_last(lambda j, peer: stat.at[1], stats1.at[tp], 12)
    last_blocks(by_sequence(weight_t * read), us1)
    push_last(lambda j, peer: us1.at[j, peer], ur1.at[tp], 10)
    update(rk, values_t, 1)
    wait_bytes(stats1, rs.at[12])
    coef = coefficients(stats1)
    coef = jnp.where(
        gj < 2,
        jnp.where(gj == 0, coef[0:4], coef[4:8]),
        jnp.where(gj == 2, coef[8:12], coef[12:16]),
    )
    wait_bytes(rest, rs.at[13])
    base = rest[...].astype(f32)
    wait_bytes(ur1, rs.at[10])
    out[...] = (base + scaled(coef, ur1)).astype(bf16)

    for ref, sem_id in sends:
        wait_bytes(ref, ss.at[sem_id])

    @pl.when(dp == res_owner)
    def _():
        wait_bytes(res_s.at[pl.ds(0, DP - 1)], ss.at[3])

    last = ((ur1, 10), (stats1, 12))

    @pl.when(lax.div(tp, ROWS) == dp)
    def _():
        for ref, sem_id in last:
            wait_bytes(ref.at[pl.ds(0, TP - 1)], ss.at[sem_id])

    @pl.when(lax.div(tp, ROWS) != dp)
    def _():
        for ref, sem_id in last:
            wait_bytes(ref, ss.at[sem_id])

    @pl.when(jnp.logical_not(rest_here))
    def _():
        wait_bytes(rest, ss.at[13])

    wait_bytes(wo0.at[0, pl.ds(0, RING - 1)], side_s)
    wait_bytes(wo0.at[0], side_s)
    wait_bytes(w1.at[0, pl.ds(0, RING - 1)], side_s)
    wait_bytes(w1.at[0], side_s)


def body(tokens, lengths, states, norm_gain, w_query, w_key, w_value, w_gate, head_gain, w_out):
    flip = lambda w: jnp.transpose(w, (0, 2, 1))
    hbm = pl.BlockSpec(memory_space=pl.ANY)
    vmem = pltpu.VMEM
    dma = pltpu.SemaphoreType.DMA
    return pl.pallas_call(
        kernel,
        out_shape=(vmem((ROWS, FEATS), bf16), vmem(states.shape, f32)),
        in_specs=[hbm] * 10,
        out_specs=(pl.BlockSpec(memory_space=vmem), pl.BlockSpec(memory_space=vmem)),
        scratch_shapes=[
            pltpu.SMEM((SEQ,), jnp.int32),
            vmem((ROWS, FEATS), bf16),
            vmem((TP, ROWS, FEATS), bf16),
            vmem((TP * ROWS, FEATS), bf16),
            vmem((DK, FEATS), bf16),
            vmem((4, COLS, FEATS), bf16),
            vmem((2, RING, COLS, FEATS), bf16),
            vmem((2, RING, PIECES, COLS, FEATS), bf16),
            vmem((LAYERS, FEATS), bf16),
            vmem((LAYERS, COLS), bf16),
            vmem((DP, SEQ, DK), bf16),
            vmem((DP, SEQ, DK), bf16),
            vmem((DP, 1, DK), f32),
            vmem((DP, 1, DK), f32),
            vmem((GROUP, SEQ, DK), bf16),
            vmem((LAYERS, 1, DK), f32),
            vmem((TP, 1, DK), f32),
            vmem((TP, 1, DK), f32),
            vmem((DP, 8, DK), bf16),
            vmem((8, DK), bf16),
            vmem((TP, 8, DK), bf16),
            vmem((TP, 8, DK), bf16),
            vmem((8, DK), bf16),
            vmem((TP, 8, DK), bf16),
            vmem((ROWS, DP, ROWS, FEATS), bf16),
            vmem((TP, ROWS, FEATS), bf16),
            vmem((ROWS, FEATS), bf16),
            vmem((ROWS, FEATS), bf16),
            vmem((GROUP, LAYERS, SEQ, DK), f32),
            vmem((GROUP, 1, FEATS), f32),
            vmem((DP, 1, FEATS), f32),
            dma((15,)),
            dma((4,)),
            dma((4,)),
            dma((3,)),
            dma,
            dma((15,)),
            dma((15,)),
        ],
        compiler_params=pltpu.CompilerParams(collective_id=0, has_side_effects=True),
        name="retention_step",
    )(
        tokens, lengths, states, norm_gain,
        flip(w_query), flip(w_key), flip(w_value), flip(w_gate), head_gain, w_out,
    )


def solution(mesh):
    placed = (
        P("tp", "dp"),
        P("dp"),
        P(None, "dp", "tp", None),
        P(None, "dp"),
        P(None, "dp", "tp"),
        P(None, "dp", "tp"),
        P(None, "dp", "tp"),
        P(None, "dp", "tp"),
        P(None, "tp"),
        P(None, "tp", "dp"),
    )
    return jax.shard_map(
        body,
        mesh=mesh,
        in_specs=placed,
        out_specs=(P("tp", "dp"), P(None, "dp", "tp", None)),
        check_vma=False,
    )
```
